256 devices in a mesh: sp: 64 (over z, y, core), tp: 4 (over x).
Axes of the slice: x: 4, y: 4, z: 8, core: 2. Of those that a mesh axis runs over, the one named last changes fastest.
Arguments:
- stream_in: bfloat16 [32768, 2048], P(('sp', 'tp')), may hold values from -6 to 6
- stream_cot: bfloat16 [32768, 2048], P(('sp', 'tp')), may hold values from -12 to 12
- route_ids: int32 [32768, 2], P('sp'), may hold values from 0 to 63, all different within a row; in each aligned block of 128 rows (0 to 127, 128 to 255, ...) at most 5 rows name the same one
- route_wts: float32 [32768, 2], P('sp'), may hold values from 0.2 to 0.8
- norm_gain: float32 [2048], replicated, may hold values from 0.1 to 1.9
- w_gate: bfloat16 [64, 2048, 1024], P('sp', None, 'tp'), may hold values from -0.125 to 0.125
- w_up: bfloat16 [64, 2048, 1024], P('sp', None, 'tp'), may hold values from -0.125 to 0.125
- w_down: bfloat16 [64, 1024, 2048], P('sp', 'tp'), may hold values from -0.1875 to 0.1875
- out_proj: bfloat16 [1024, 2048], P('tp'), may hold values from -0.1875 to 0.1875
- conv_b: bfloat16 [32768, 1024], P('sp', 'tp'), may hold values from -6 to 6
- conv_c: bfloat16 [32768, 1024], P('sp', 'tp'), may hold values from -6 to 6
- conv_h: bfloat16 [32768, 1024], P('sp', 'tp'), may hold values from -6 to 6
- conv_taps: float32 [3, 1024], P(None, 'tp'), may hold values from -3.5 to 3.5
Outputs:
- grad_gate: float32 [64, 2048, 1024], P('sp', None, 'tp')
- grad_up: float32 [64, 2048, 1024], P('sp', None, 'tp')
- grad_down: float32 [64, 1024, 2048], P('sp', 'tp')
- proj_grad: float32 [2048, 1024], P('sp', 'tp')
- grad_b: bfloat16 [32768, 1024], P('sp', 'tp')
- grad_c: bfloat16 [32768, 1024], P('sp', 'tp')
- grad_h: bfloat16 [32768, 1024], P('sp', 'tp')
The draws below stay inside these ranges and needn't reach their ends.
Inputs may be any that keep to these rules, and one draw needn't show every extreme that they name: `route_ids`: the 2 experts of a token differ. In each aligned block of 128 tokens no expert is named by more than 5 pairs, and in every draw some expert is named by exactly 5 pairs of some block.
All inputs are finite; a program needn't handle non-finite values.
Results may differ from the reference program's by a relative error of at most 0.015.
Values may be sent and summed in bfloat16 or wider, within the bound.
No kernel may reach another device: no remote copies, remote signals or barrier semaphores. Data moves between devices by JAX's collectives and lax.ppermute only.
A program may use at most 128 MiB of HBM per device.

```python
import math
import jax
import jax.numpy as jnp
import numpy as np
from jax import lax

D = 2048
SC_W = 1024
FF = 1024
TOPK = 2
TAPS = 3
TOK_DEV = 128
TOKENS = 32768
EXPERTS = 64
CAP = 5
N_SP = 64
N_TP = 4


def raised(drawn, rng, source, target, shards_of, factor):
    owner, partner = [(jnp.arange(drawn.shape[axis_at]) // (drawn.shape[axis_at] // shards_of)).reshape([-1 if axis == axis_at else 1 for axis in range(drawn.ndim)]) for axis_at in (source, target)]
    chosen = jax.random.permutation(rng, shards_of)[partner]
    strong = (owner == chosen) | (owner == (partner + shards_of // 2) % shards_of)
    return jnp.where(strong, factor * drawn, drawn)


def block_levels(rng, shape, split, least, largest):
    gain, own = 1.0, jax.random.fold_in(rng, 6)
    for dim, parts in split:
        draws = jnp.exp(jax.random.uniform(jax.random.fold_in(own, dim), (parts,), jnp.float32, least / len(split), largest / len(split)))
        gain = gain * jnp.repeat(draws, shape[dim] // parts).reshape([-1 if axis == dim else 1 for axis in range(len(shape))])
    return gain


def deal_out(own_key, own, number, rows, count, top, limit, lean):
    ranking = jax.random.permutation(own_key, count)
    crowded, ordinary = portions_of(count, rows * top, limit, lean, True), portions_of(count, rows * top, limit, lean, False)
    places = jnp.arange(count)

    def named(sizes, rotation):
        used = int((sizes > 0).sum())
        fixed = max(1, used // 4)
        passed = fixed + (places - fixed + rotation * (used - fixed)) % max(1, count - fixed)
        return jnp.zeros((count,), jnp.int32).at[ranking[jnp.where(places < fixed, places, passed)]].set(jnp.asarray(sizes, jnp.int32))

    sizes = jnp.where(number % 4 == 0, named(crowded, number // 4), named(ordinary, number - number // 4 - 1))
    mixed = jax.random.permutation(jax.random.fold_in(own, 3), count)
    source_of, taker = mixed[0:count // 2 * 2:2], mixed[1:count // 2 * 2:2]
    slack = jnp.minimum(sizes[source_of] - 1, limit - sizes[taker]) // 2
    slack = jnp.where((source_of == ranking[0]) | (taker == ranking[0]) | (sizes[taker] == 0), 0, jnp.maximum(slack, 0))
    passed = jax.random.randint(jax.random.fold_in(own, 4), (count // 2,), 0, 1 << 20) % (slack + 1)
    sizes = sizes.at[source_of].add(-passed).at[taker].add(passed)
    members = jnp.searchsorted(jnp.cumsum(sizes), jnp.arange(rows * top), side="right").astype(jnp.int32)
    table = members.reshape(top, rows).T
    table = table[jax.random.permutation(jax.random.fold_in(own, 1), rows)]
    rotation = jax.random.randint(jax.random.fold_in(own, 2), (rows, 1), 0, top)
    return jnp.take_along_axis(table, (jnp.arange(top)[None, :] + rotation) % top, axis=1)


def portions_of(count, total, most, lean, full):
    portions = [(1 << 20) // math.isqrt(rank ** lean) + 1 for rank in range(1, count + 1)]
    largest = most if full else min(most, max(-(-total // count), total * portions[0] // sum(portions)))
    least = 1 if total - largest >= count - 1 else 0
    counts, rest = [largest] + [least] * (count - 1), total - largest - least * (count - 1)
    while rest > 0:
        candidates = [i for i in range(1, count) if counts[i] < largest] or [i for i in range(1, count) if counts[i] < most]
        mass, budget = sum([portions[i] for i in candidates]), rest
        for i in candidates:
            extra = min(most - counts[i], max(1, budget * portions[i] // mass), rest)
            counts[i] = counts[i] + extra
            rest = rest - extra
    return np.array(counts)


def scatter_about(rng, shape, spread, most, cuts=(), held_as=jnp.bfloat16):
    gain = block_levels(rng, shape, cuts, -0.22, 0.18) if cuts else 1.0
    array = jax.random.normal(rng, shape, jnp.float32) * spread * gain
    return jnp.minimum(jnp.maximum(array, -most), most).astype(held_as)


def noise_with(own_key, dims, scale, most, cuts, heavy, held_as=jnp.bfloat16):
    values = scale * jax.random.normal(own_key, dims, jnp.float32)
    if cuts:
        values = values * block_levels(own_key, dims, cuts, -0.22, 0.18)
    return jnp.clip(raised(values, jax.random.fold_in(own_key, 3), *heavy), -most, most).astype(held_as)


def setup_inputs(seed: int = 0) -> dict:
    key_list = jax.random.split(jax.random.key(seed), 14)
    stream_in = scatter_about(key_list[0], (TOKENS, D), 1.0, 6.0, ((0, 256),))
    stream_cot = noise_with(key_list[1], (TOKENS, D), 0.5, 12.0, ((0, 256),), (0, 1, 256, 6.0))
    route_ids_keys = jax.random.split(jax.random.fold_in(key_list[2], 1), TOKENS // TOK_DEV)
    route_ids_turns = jax.random.permutation(jax.random.fold_in(key_list[2], 3), TOKENS // TOK_DEV)
    route_ids = jax.vmap(lambda own, number: deal_out(jax.random.fold_in(key_list[2], 2), own, number, TOK_DEV, EXPERTS, TOPK, CAP, 1))(route_ids_keys, route_ids_turns).reshape((TOKENS, TOPK))
    route_wts = jnp.clip(0.2 + 0.6 * jax.random.uniform(key_list[3], (TOKENS, TOPK), jnp.float32) ** block_levels(key_list[3], (TOKENS, TOPK), ((0, 64),), -0.2, 0.2), 0.2, 0.8)
    norm_gain = jnp.clip(1.0 + 0.18 * jax.random.normal(key_list[4], (D,), jnp.float32), 0.1, 1.9)
    w_gate = scatter_about(key_list[5], (EXPERTS, D, FF), D ** -0.5, 0.125, ((0, 64), (2, 4)))
    w_up = scatter_about(key_list[6], (EXPERTS, D, FF), D ** -0.5, 0.125, ((0, 64), (2, 4)))
    w_down = scatter_about(key_list[7], (EXPERTS, FF, D), FF ** -0.5, 0.1875, ((0, 64), (1, 4)))
    out_proj = scatter_about(key_list[8], (SC_W, D), SC_W ** -0.5, 0.1875, ((0, 4),))
    conv_b = scatter_about(key_list[9], (TOKENS, SC_W), 1.0, 6.0, ((0, 64), (1, 4)))
    conv_c = scatter_about(key_list[10], (TOKENS, SC_W), 1.0, 6.0, ((0, 64), (1, 4)))
    conv_h = scatter_about(key_list[11], (TOKENS, SC_W), 1.0, 6.0, ((0, 64), (1, 4)))
    conv_taps = scatter_about(key_list[12], (TAPS, SC_W), TAPS ** -0.5, 3.5, ((1, 4),), jnp.float32)
    return dict(stream_in=stream_in, stream_cot=stream_cot, route_ids=route_ids, route_wts=route_wts, norm_gain=norm_gain, w_gate=w_gate, w_up=w_up, w_down=w_down, out_proj=out_proj, conv_b=conv_b, conv_c=conv_c, conv_h=conv_h, conv_taps=conv_taps)


epsilon = 1e-06

def rounded(value):
    return lax.optimization_barrier(value.astype(jnp.bfloat16)).astype(jnp.float32)

def mmul(left, right):
    return jnp.dot(left, right, precision=lax.Precision.HIGHEST)

def reference(stream_in, stream_cot, route_ids, route_wts, norm_gain, w_gate, w_up, w_down, out_proj, conv_b, conv_c, conv_h, conv_taps):
    inputs = stream_in.astype(jnp.float32)
    inv_rms = lax.rsqrt(lax.optimization_barrier(jnp.mean(inputs * inputs, axis=1, keepdims=True)) + epsilon)
    scaled = inputs * inv_rms
    normed = (scaled * norm_gain[None, :]).astype(jnp.bfloat16)
    device_count = N_SP * N_TP
    pair_count = TOPK * TOKENS
    ids_device = route_ids.reshape(device_count, TOPK * TOK_DEV)
    onehot = (ids_device[:, :, None] == jnp.arange(EXPERTS, dtype=jnp.int32)).astype(jnp.int32)
    slot_rank = lax.optimization_barrier(jnp.sum((jnp.cumsum(onehot, axis=1) - 1) * onehot, axis=2))
    device_idx = jnp.arange(device_count, dtype=jnp.int32)[:, None]
    per_expert = device_count * CAP
    position = ids_device * per_expert + device_idx * CAP + slot_rank
    slot_table = jnp.full((EXPERTS * per_expert,), pair_count, jnp.int32)
    slot_table = slot_table.at[position.reshape(-1)].set(jnp.arange(pair_count, dtype=jnp.int32))
    slot_table = slot_table.reshape(EXPERTS, per_expert)
    zero_row = jnp.zeros((1, D), jnp.bfloat16)
    normed_pad = jnp.concatenate([normed, zero_row], axis=0)
    cot_pad = jnp.concatenate([stream_cot, zero_row], axis=0)
    wts_pad = jnp.concatenate([route_wts.reshape(-1), jnp.zeros((1,), jnp.float32)])
    ff_block = FF // N_TP

    def one_expert(grad_total, expert_in):
        pair_rows, gate_w, up_w, down_w = expert_in
        token_rows = pair_rows // TOPK
        rows_in = normed_pad[token_rows].astype(jnp.float32)
        cot_rows = rounded(wts_pad[pair_rows][:, None] * cot_pad[token_rows].astype(jnp.float32))
        gate_f = gate_w.astype(jnp.float32)
        up_f = up_w.astype(jnp.float32)
        down_f = down_w.astype(jnp.float32)
        gate_pre = mmul(rows_in, gate_f)
        up_pre = mmul(rows_in, up_f)
        gate_sig = jax.nn.sigmoid(gate_pre)
        gate_act = gate_pre * gate_sig
        hidden = rounded(gate_act * up_pre)
        down_grad = mmul(hidden.T, cot_rows)
        grad_hidden = mmul(cot_rows, down_f.T)
        up_grad = rounded(grad_hidden * gate_act)
        gate_grad = rounded(grad_hidden * up_pre * gate_sig * (1.0 + gate_pre * (1.0 - gate_sig)))
        gate_wgrad = mmul(rows_in.T, gate_grad)
        up_wgrad = mmul(rows_in.T, up_grad)
        back_sum = jnp.zeros((rows_in.shape[0], D), jnp.float32)
        for block_idx in range(N_TP):
            low = block_idx * ff_block
            high = low + ff_block
            partial_back = mmul(gate_grad[:, low:high], gate_f[:, low:high].T) + mmul(up_grad[:, low:high], up_f[:, low:high].T)
            back_sum = back_sum + rounded(partial_back)
        back_rows = rounded(back_sum)
        grad_total = grad_total.at[token_rows].add(back_rows)
        return (grad_total, (gate_wgrad, up_wgrad, down_grad))
    start_total = jnp.zeros((TOKENS + 1, D), jnp.float32)
    grad_total, expert_grads = lax.scan(one_expert, start_total, (slot_table, w_gate, w_up, w_down))
    grad_gate, grad_up, grad_down = expert_grads
    grad_normed = grad_total[:TOKENS]
    q_term = grad_normed * norm_gain[None, :]
    stream_grad = (stream_cot.astype(jnp.float32) + inv_rms * (q_term - scaled * lax.optimization_barrier(jnp.mean(q_term * scaled, axis=1, keepdims=True)))).astype(jnp.bfloat16)
    grad_mix = jnp.dot(stream_grad, out_proj.T, preferred_element_type=jnp.float32).astype(jnp.bfloat16)
    conv_in = conv_c.astype(jnp.float32) * conv_h.astype(jnp.float32)
    padded_in = jnp.pad(conv_in, ((2, 0), (0, 0)))
    conv_out = conv_taps[0][None, :] * padded_in[:-2] + conv_taps[1][None, :] * padded_in[1:-1] + conv_taps[2][None, :] * padded_in[2:]
    mixed = (conv_b.astype(jnp.float32) * conv_out).astype(jnp.bfloat16)
    proj_grad = jnp.dot(stream_grad.T, mixed, preferred_element_type=jnp.float32)
    grad_b = (grad_mix.astype(jnp.float32) * conv_out).astype(jnp.bfloat16)
    conv_grad = grad_mix.astype(jnp.float32) * conv_b.astype(jnp.float32)
    padded_grad = jnp.pad(conv_grad, ((0, 2), (0, 0)))
    grad_in = conv_taps[2][None, :] * padded_grad[:-2] + conv_taps[1][None, :] * padded_grad[1:-1] + conv_taps[0][None, :] * padded_grad[2:]
    grad_c = (grad_in * conv_h.astype(jnp.float32)).astype(jnp.bfloat16)
    grad_h = (grad_in * conv_c.astype(jnp.float32)).astype(jnp.bfloat16)
    return (grad_gate, grad_up, grad_down, proj_grad, grad_b, grad_c, grad_h)
```

```python
import jax
import jax.numpy as jnp
from jax import lax
from jax.sharding import Mesh, PartitionSpec as P

epsilon = 1e-06
SP = ("z", "y", "c")
bf16 = jnp.bfloat16
f32 = jnp.float32


def shift(x, axis, steps):
    count = lax.axis_size(axis)
    return lax.ppermute(x, axis, [(i, (i + steps) % count) for i in range(count)])


def from_behind(value, axis, steps):
    count = lax.axis_size(axis)
    initial, last = (max(0, -steps), min(count, count - steps))
    return lax.ppermute(value, axis, [(source, source + steps) for source in range(initial, last)])


def exchange(x, axis):
    return lax.all_to_all(x, axis, split_axis=0, concat_axis=0, tiled=True)


def ring_gather(x):
    half = x.shape[0] // 2
    left = shift(x, "tp", 1)
    right = shift(x, "tp", -1)
    far_a = shift(left[:half], "tp", 1)
    far_b = shift(right[half:], "tp", -1)
    return x, left, right, far_a, far_b


def ring_reduce(own, left, right, far):
    half = own.shape[0] // 2
    from_left = shift(far[:half], "tp", 1)
    from_right = shift(far[half:], "tp", -1)
    right_a = (right[:half].astype(f32) + from_left.astype(f32)).astype(bf16)
    left_b = (left[half:].astype(f32) + from_right.astype(f32)).astype(bf16)
    l_b = shift(right[half:], "tp", 1)
    r_a = shift(left[:half], "tp", -1)
    l_a = shift(right_a, "tp", 1)
    r_b = shift(left_b, "tp", -1)
    top = own[:half].astype(f32) + l_a.astype(f32) + r_a.astype(f32)
    low = own[half:].astype(f32) + l_b.astype(f32) + r_b.astype(f32)
    return jnp.concatenate([top, low], axis=0).astype(bf16)


def dot(a, b, ca, cb):
    return lax.dot_general(a, b, (((ca,), (cb,)), ((), ())), preferred_element_type=f32)


def sent_over(x, sp_count):
    slots, width = x.shape
    rows = x.reshape(sp_count, slots // sp_count * (width // 128), 128)
    return exchange(rows, SP).reshape(slots, width)


def shards(
    stream_in,
    stream_cot,
    route_ids,
    route_wts,
    norm_gain,
    w_gate,
    w_up,
    w_down,
    out_proj,
    conv_b,
    conv_c,
    conv_h,
    conv_taps,
):
    tp_count = lax.axis_size("tp")
    sp_count = lax.axis_size(SP)
    tp_index = lax.axis_index("tp")
    tok_rows, model_width = stream_in.shape
    top_count = route_ids.shape[1]
    capacity = max(2, 5 * top_count * tok_rows // (4 * sp_count))
    slots = sp_count * capacity
    halves = 2
    part = model_width // halves
    cols = [slice(i * part, (i + 1) * part) for i in range(halves)]
    w_gate, w_up, w_down = w_gate[0], w_up[0], w_down[0]

    inputs = stream_in.astype(f32)
    inv_rms = lax.rsqrt(jnp.mean(inputs * inputs, axis=1, keepdims=True) + epsilon)
    scaled = inputs * inv_rms
    normed = (scaled * norm_gain[None, :]).astype(bf16)

    own_ids = lax.dynamic_slice_in_dim(route_ids, tp_index * tok_rows, tok_rows, 0)
    own_wts = lax.dynamic_slice_in_dim(route_wts, tp_index * tok_rows, tok_rows, 0)
    experts = jnp.arange(sp_count, dtype=jnp.int32)
    marks = [own_ids[:, k : k + 1] == experts[None, :] for k in range(top_count)]
    any_mark = sum(m.astype(bf16) for m in marks)
    index = jnp.arange(tok_rows, dtype=jnp.int32)
    before = (index[:, None] > index[None, :]).astype(bf16)
    ranks = dot(before, any_mark, 1, 0)
    places = [
        own_ids[:, k] * capacity
        + jnp.sum(jnp.where(marks[k], ranks, 0.0), axis=1).astype(jnp.int32)
        for k in range(top_count)
    ]
    slot_index = jnp.arange(slots, dtype=jnp.int32)
    picks = [slot_index[:, None] == places[k][None, :] for k in range(top_count)]
    select = sum(p.astype(bf16) for p in picks)
    slot_wts = sum(
        jnp.sum(jnp.where(picks[k], own_wts[:, k][None, :], 0.0), axis=1, keepdims=True)
        for k in range(top_count)
    )
    slot_rows = [dot(select, normed[:, c], 1, 0).astype(bf16) for c in cols]
    slot_cot = [(slot_wts * dot(select, stream_cot[:, c], 1, 0)).astype(bf16) for c in cols]

    landed_rows = [sent_over(x, sp_count) for x in slot_rows]
    landed_cot = [sent_over(x, sp_count) for x in slot_cot]
    rows = [jnp.concatenate(ring_gather(x), axis=0) for x in landed_rows]
    cots = [jnp.concatenate(ring_gather(x), axis=0) for x in landed_cot]

    gate_pre = sum(dot(r, w_gate[c], 1, 0) for r, c in zip(rows, cols))
    up_pre = sum(dot(r, w_up[c], 1, 0) for r, c in zip(rows, cols))
    gate_sig = jax.nn.sigmoid(gate_pre)
    gate_act = gate_pre * gate_sig
    hidden = (gate_act * up_pre).astype(bf16)
    grad_hidden = sum(dot(r, w_down[:, c], 1, 1) for r, c in zip(cots, cols))
    up_grad = (grad_hidden * gate_act).astype(bf16)
    gate_grad = (grad_hidden * up_pre * gate_sig * (1.0 + gate_pre * (1.0 - gate_sig))).astype(bf16)

    returned = []
    for c in cols:
        back = (dot(gate_grad, w_gate[c], 1, 1) + dot(up_grad, w_up[c], 1, 1)).astype(bf16)
        back = [back[i * slots : (i + 1) * slots] for i in range(tp_count)]
        returned.append(sent_over(ring_reduce(*back), sp_count))
    gate_wgrad = jnp.concatenate([dot(r, gate_grad, 0, 0) for r in rows], axis=0)
    up_wgrad = jnp.concatenate([dot(r, up_grad, 0, 0) for r in rows], axis=0)
    down_grad = jnp.concatenate([dot(hidden, r, 0, 0) for r in cots], axis=1)

    grad_normed = jnp.concatenate([dot(select, r, 0, 0) for r in returned], axis=1)
    q_term = grad_normed * norm_gain[None, :]
    stream_grad = (
        stream_cot.astype(f32)
        + inv_rms * (q_term - scaled * jnp.mean(q_term * scaled, axis=1, keepdims=True))
    ).astype(bf16)
    own, left, right, far_a, far_b = ring_gather(stream_grad)
    group_grad = jnp.concatenate([own, right, far_a, far_b, left], axis=0)
    mix_turned = dot(group_grad, out_proj, 1, 1).astype(bf16)

    def turned(x, by):
        twice = jnp.concatenate([x, x], axis=0)
        return lax.dynamic_slice_in_dim(twice, by * tok_rows, tp_count * tok_rows, 0)

    grad_mix = turned(mix_turned, (tp_count - tp_index) % tp_count)

    rim_prev = from_behind(jnp.stack([conv_c[-2:], conv_h[-2:]]), SP, 1)
    gate_ext = jnp.concatenate([rim_prev[0], conv_c], axis=0).astype(f32)
    value_ext = jnp.concatenate([rim_prev[1], conv_h], axis=0).astype(f32)
    conv_in = gate_ext * value_ext
    conv_out = (
        conv_taps[0][None, :] * conv_in[:-2]
        + conv_taps[1][None, :] * conv_in[1:-1]
        + conv_taps[2][None, :] * conv_in[2:]
    )
    mixed = turned((conv_b.astype(f32) * conv_out).astype(bf16), tp_index)

    proj = dot(group_grad, mixed, 0, 0)
    nz, ny, nc = (lax.axis_size(a) for a in SP)
    own_depth = model_width // sp_count
    width = proj.shape[1]
    proj = proj.reshape(nz * ny, nc, own_depth, width).astype(bf16)
    proj = exchange(jnp.moveaxis(proj, 1, 0), "c")
    proj = proj.astype(f32).sum(axis=0).astype(bf16)
    proj = jnp.moveaxis(proj.reshape(nz, ny, own_depth, width), 1, 0)
    proj = exchange(proj, "y").astype(f32).sum(axis=0).astype(bf16)
    proj_grad = exchange(proj, "z").astype(f32).sum(axis=0)

    grad_b = (grad_mix.astype(f32) * conv_out).astype(bf16)
    rim_next = from_behind(jnp.stack([grad_mix[:2], conv_b[:2]]), SP, -1)
    conv_grad = grad_mix.astype(f32) * conv_b.astype(f32)
    next_grad = rim_next[0].astype(f32) * rim_next[1].astype(f32)
    grad_ext = jnp.concatenate([conv_grad, next_grad], axis=0)
    grad_in = (
        conv_taps[2][None, :] * grad_ext[:-2]
        + conv_taps[1][None, :] * grad_ext[1:-1]
        + conv_taps[0][None, :] * grad_ext[2:]
    )
    grad_c = (grad_in * conv_h.astype(f32)).astype(bf16)
    grad_h = (grad_in * conv_c.astype(f32)).astype(bf16)
    return (gate_wgrad[None], up_wgrad[None], down_grad[None], proj_grad, grad_b, grad_c, grad_h)


def solution(mesh):
    split = Mesh(mesh.devices.reshape(8, 4, 2, 4), (*SP, "tp"))
    in_specs = (
        P((*SP, "tp"), None),
        P((*SP, "tp"), None),
        P(SP, None),
        P(SP, None),
        P(),
        P(SP, None, "tp"),
        P(SP, None, "tp"),
        P(SP, "tp", None),
        P("tp", None),
        P(SP, "tp"),
        P(SP, "tp"),
        P(SP, "tp"),
        P(None, "tp"),
    )
    out_specs = (
        P(SP, None, "tp"),
        P(SP, None, "tp"),
        P(SP, "tp", None),
        P(SP, "tp"),
        P(SP, "tp"),
        P(SP, "tp"),
        P(SP, "tp"),
    )
    return jax.shard_map(shards, mesh=split, in_specs=in_specs, out_specs=out_specs, check_vma=False)
```

```python
import jax
import jax.numpy as jnp
from jax import lax
from jax.sharding import Mesh, PartitionSpec as P


epsilon = 1e-06
SP = ("z", "y", "c")
bf16 = jnp.bfloat16
f32 = jnp.float32


def shift(x, axis, steps):
    count = lax.axis_size(axis)
    return lax.ppermute(x, axis, [(i, (i + steps) % count) for i in range(count)])


def from_behind(value, axis, steps):
    count = lax.axis_size(axis)
    initial, last = (max(0, -steps), min(count, count - steps))
    return lax.ppermute(value, axis, [(source, source + steps) for source in range(initial, last)])


def exchange(x, axis):
    return lax.all_to_all(x, axis, split_axis=0, concat_axis=0, tiled=True)


def ring_gather(x):
    half = x.shape[0] // 2
    left = shift(x, "tp", 1)
    right = shift(x, "tp", -1)
    far_a = shift(left[:half], "tp", 1)
    far_b = shift(right[half:], "tp", -1)
    return x, left, right, far_a, far_b


def joined(pieces):
    own, left, right, far_a, far_b = pieces
    return own, left, right, jnp.concatenate([far_a, far_b], axis=0)


def ring_reduce(own, left, right, far):
    half = own.shape[0] // 2
    from_left = shift(far[:half], "tp", 1)
    from_right = shift(far[half:], "tp", -1)
    right_a = (right[:half].astype(f32) + from_left.astype(f32)).astype(bf16)
    left_b = (left[half:].astype(f32) + from_right.astype(f32)).astype(bf16)
    l_b = shift(right[half:], "tp", 1)
    r_a = shift(left[:half], "tp", -1)
    l_a = shift(right_a, "tp", 1)
    r_b = shift(left_b, "tp", -1)
    top = own[:half].astype(f32) + l_a.astype(f32) + r_a.astype(f32)
    low = own[half:].astype(f32) + l_b.astype(f32) + r_b.astype(f32)
    return jnp.concatenate([top, low], axis=0).astype(bf16)


def dot(a, b, ca, cb):
    return lax.dot_general(a, b, (((ca,), (cb,)), ((), ())), preferred_element_type=f32)


def sent_over(x, sp_count):
    slots, width = x.shape
    rows = x.reshape(sp_count, slots // sp_count * (width // 128), 128)
    return exchange(rows, SP).reshape(slots, width)


def step(
    stream_in,
    stream_cot,
    route_ids,
    route_wts,
    norm_gain,
    w_gate,
    w_up,
    w_down,
    out_proj,
    conv_b,
    conv_c,
    conv_h,
    conv_taps,
):
    tp_count = lax.axis_size("tp")
    sp_count = lax.axis_size(SP)
    tp_index = lax.axis_index("tp")
    tok_rows, model_width = stream_in.shape
    top_count = route_ids.shape[1]
    capacity = max(2, 5 * top_count * tok_rows // (4 * sp_count))
    slots = sp_count * capacity
    halves = 2
    part = model_width // halves
    cols = [slice(i * part, (i + 1) * part) for i in range(halves)]
    w_gate, w_up, w_down = w_gate[0], w_up[0], w_down[0]

    inputs = stream_in.astype(f32)
    inv_rms = lax.rsqrt(jnp.mean(inputs * inputs, axis=1, keepdims=True) + epsilon)
    scaled = inputs * inv_rms
    normed = (scaled * norm_gain[None, :]).astype(bf16)

    own_ids = lax.dynamic_slice_in_dim(route_ids, tp_index * tok_rows, tok_rows, 0)
    own_wts = lax.dynamic_slice_in_dim(route_wts, tp_index * tok_rows, tok_rows, 0)
    experts = jnp.arange(sp_count, dtype=jnp.int32)
    marks = [own_ids[:, k : k + 1] == experts[None, :] for k in range(top_count)]
    any_mark = sum(m.astype(bf16) for m in marks)
    index = jnp.arange(tok_rows, dtype=jnp.int32)
    before = (index[:, None] > index[None, :]).astype(bf16)
    ranks = dot(before, any_mark, 1, 0)
    places = [
        own_ids[:, k] * capacity
        + jnp.sum(jnp.where(marks[k], ranks, 0.0), axis=1).astype(jnp.int32)
        for k in range(top_count)
    ]
    slot_index = jnp.arange(slots, dtype=jnp.int32)
    picks = [slot_index[:, None] == places[k][None, :] for k in range(top_count)]
    select = sum(p.astype(bf16) for p in picks)
    slot_wts = sum(
        jnp.sum(jnp.where(picks[k], own_wts[:, k][None, :], 0.0), axis=1, keepdims=True)
        for k in range(top_count)
    )
    slot_rows = dot(select, normed, 1, 0).astype(bf16)
    slot_cot = (slot_wts * dot(select, stream_cot, 1, 0)).astype(bf16)

    down_all = joined(ring_gather(w_down))
    landed_rows = sent_over(slot_rows, sp_count)
    landed_cot = sent_over(slot_cot, sp_count)
    rows = joined(ring_gather(landed_rows))

    mine = [dot(landed_cot, w, 1, 1) for w in down_all]
    grad_hidden = [
        mine[0],
        shift(mine[2].astype(bf16), "tp", 1).astype(f32),
        shift(mine[1].astype(bf16), "tp", -1).astype(f32),
        shift(mine[3].astype(bf16), "tp", 2).astype(f32),
    ]
    hidden, up_grad, gate_grad = [], [], []
    for r, g in zip(rows, grad_hidden):
        gate_pre = dot(r, w_gate, 1, 0)
        up_pre = dot(r, w_up, 1, 0)
        gate_sig = jax.nn.sigmoid(gate_pre)
        gate_act = gate_pre * gate_sig
        hidden.append((gate_act * up_pre).astype(bf16))
        up_grad.append((g * gate_act).astype(bf16))
        gate_grad.append((g * up_pre * gate_sig * (1.0 + gate_pre * (1.0 - gate_sig))).astype(bf16))

    returned = []
    for c in cols:
        back = [
            (dot(gg, w_gate[c], 1, 1) + dot(ug, w_up[c], 1, 1)).astype(bf16)
            for gg, ug in zip(gate_grad, up_grad)
        ]
        summed = ring_reduce(*back)
        returned.append(sent_over(summed, sp_count))
    cots = jnp.concatenate(ring_gather(landed_cot), axis=0)
    all_rows = jnp.concatenate(rows, axis=0)
    gate_wgrad = dot(all_rows, jnp.concatenate(gate_grad, axis=0), 0, 0)
    up_wgrad = dot(all_rows, jnp.concatenate(up_grad, axis=0), 0, 0)
    down_grad = dot(jnp.concatenate(hidden, axis=0), cots, 0, 0)

    grad_normed = jnp.concatenate([dot(select, r, 0, 0) for r in returned], axis=1)
    q_term = grad_normed * norm_gain[None, :]
    stream_grad = (
        stream_cot.astype(f32)
        + inv_rms * (q_term - scaled * jnp.mean(q_term * scaled, axis=1, keepdims=True))
    ).astype(bf16)
    own, left, right, far_a, far_b = ring_gather(stream_grad)
    group_grad = jnp.concatenate([own, right, far_a, far_b, left], axis=0)
    mix_turned = dot(group_grad, out_proj, 1, 1).astype(bf16)

    def turned(x, by):
        twice = jnp.concatenate([x, x], axis=0)
        return lax.dynamic_slice_in_dim(twice, by * tok_rows, tp_count * tok_rows, 0)

    grad_mix = turned(mix_turned, (tp_count - tp_index) % tp_count)

    rim_prev = from_behind(jnp.stack([conv_c[-2:], conv_h[-2:]]), SP, 1)
    gate_ext = jnp.concatenate([rim_prev[0], conv_c], axis=0).astype(f32)
    value_ext = jnp.concatenate([rim_prev[1], conv_h], axis=0).astype(f32)
    conv_in = gate_ext * value_ext
    conv_out = (
        conv_taps[0][None, :] * conv_in[:-2]
        + conv_taps[1][None, :] * conv_in[1:-1]
        + conv_taps[2][None, :] * conv_in[2:]
    )
    mixed = turned((conv_b.astype(f32) * conv_out).astype(bf16), tp_index)

    proj = dot(group_grad, mixed, 0, 0)
    nz, ny, nc = (lax.axis_size(a) for a in SP)
    own_depth = model_width // sp_count
    width = proj.shape[1]
    proj = proj.reshape(nz * ny, nc, own_depth, width).astype(bf16)
    proj = exchange(jnp.moveaxis(proj, 1, 0), "c")
    proj = proj.astype(f32).sum(axis=0).astype(bf16)
    proj_grad = exchange(proj, ("z", "y")).astype(f32).sum(axis=0)

    grad_b = (grad_mix.astype(f32) * conv_out).astype(bf16)
    rim_next = from_behind(jnp.stack([grad_mix[:2], conv_b[:2]]), SP, -1)
    conv_grad = grad_mix.astype(f32) * conv_b.astype(f32)
    next_grad = rim_next[0].astype(f32) * rim_next[1].astype(f32)
    grad_ext = jnp.concatenate([conv_grad, next_grad], axis=0)
    grad_in = (
        conv_taps[2][None, :] * grad_ext[:-2]
        + conv_taps[1][None, :] * grad_ext[1:-1]
        + conv_taps[0][None, :] * grad_ext[2:]
    )
    grad_c = (grad_in * conv_h.astype(f32)).astype(bf16)
    grad_h = (grad_in * conv_c.astype(f32)).astype(bf16)
    return (gate_wgrad[None], up_wgrad[None], down_grad[None], proj_grad, grad_b, grad_c, grad_h)


def solution(mesh):
    split = Mesh(mesh.devices.reshape(8, 4, 2, 4), (*SP, "tp"))
    in_specs = (
        P((*SP, "tp"), None),
        P((*SP, "tp"), None),
        P(SP, None),
        P(SP, None),
        P(),
        P(SP, None, "tp"),
        P(SP, None, "tp"),
        P(SP, "tp", None),
        P("tp", None),
        P(SP, "tp"),
        P(SP, "tp"),
        P(SP, "tp"),
        P(None, "tp"),
    )
    out_specs = (
        P(SP, None, "tp"),
        P(SP, None, "tp"),
        P(SP, "tp", None),
        P(SP, "tp"),
        P(SP, "tp"),
        P(SP, "tp"),
        P(SP, "tp"),
    )
    return jax.shard_map(step, mesh=split, in_specs=in_specs, out_specs=out_specs, check_vma=False)
```

```python
import jax
import jax.numpy as jnp
from jax import lax
from jax.sharding import Mesh, PartitionSpec as P


epsilon = 1e-06
SP = ("z", "y", "c")
bf16 = jnp.bfloat16
f32 = jnp.float32


def shift(x, axis, steps):
    count = lax.axis_size(axis)
    return lax.ppermute(x, axis, [(i, (i + steps) % count) for i in range(count)])


def from_behind(value, axis, steps):
    count = lax.axis_size(axis)
    initial, last = (max(0, -steps), min(count, count - steps))
    return lax.ppermute(value, axis, [(source, source + steps) for source in range(initial, last)])


def exchange(x, axis):
    return lax.all_to_all(x, axis, split_axis=0, concat_axis=0, tiled=True)


def ring_gather(x):
    half = x.shape[0] // 2
    a, b = x[:half], x[half:]
    left_a = shift(a, "tp", 1)
    right_b = shift(b, "tp", -1)
    left_b = shift(b, "tp", 1)
    right_a = shift(a, "tp", -1)
    far_a = shift(left_a, "tp", 1)
    far_b = shift(right_b, "tp", -1)
    return x, (left_a, left_b), (right_a, right_b), (far_a, far_b)


def late_gather(x):
    half = x.shape[0] // 2
    left = shift(x, "tp", 1)
    right = shift(x, "tp", -1)
    far_a = shift(left[:half], "tp", 1)
    far_b = shift(right[half:], "tp", -1)
    return jnp.concatenate([x, left, right, far_a, far_b], axis=0)


def ring_reduce(own, left, right, far):
    half = own.shape[0] // 2
    from_left = shift(far[:half], "tp", 1)
    from_right = shift(far[half:], "tp", -1)
    right_a = (right[:half].astype(f32) + from_left.astype(f32)).astype(bf16)
    left_b = (left[half:].astype(f32) + from_right.astype(f32)).astype(bf16)
    l_b = shift(right[half:], "tp", 1)
    r_a = shift(left[:half], "tp", -1)
    l_a = shift(right_a, "tp", 1)
    r_b = shift(left_b, "tp", -1)
    top = own[:half].astype(f32) + l_a.astype(f32) + r_a.astype(f32)
    low = own[half:].astype(f32) + l_b.astype(f32) + r_b.astype(f32)
    return jnp.concatenate([top, low], axis=0).astype(bf16)


def dot(a, b, ca, cb):
    return lax.dot_general(a, b, (((ca,), (cb,)), ((), ())), preferred_element_type=f32)


def packed(x, sp_count):
    slots, width = x.shape
    return x.reshape(sp_count, slots // sp_count * (width // 128), 128)


def sent_over(x, sp_count):
    return exchange(packed(x, sp_count), SP).reshape(x.shape)


def step(
    stream_in,
    stream_cot,
    route_ids,
    route_wts,
    norm_gain,
    w_gate,
    w_up,
    w_down,
    out_proj,
    conv_b,
    conv_c,
    conv_h,
    conv_taps,
):
    tp_count = lax.axis_size("tp")
    sp_count = lax.axis_size(SP)
    tp_index = lax.axis_index("tp")
    tok_rows, model_width = stream_in.shape
    top_count = route_ids.shape[1]
    capacity = max(2, 5 * top_count * tok_rows // (4 * sp_count))
    slots = sp_count * capacity
    halves = 2
    part = model_width // halves
    cols = [slice(i * part, (i + 1) * part) for i in range(halves)]
    w_gate, w_up, w_down = w_gate[0], w_up[0], w_down[0]

    inputs = stream_in.astype(f32)
    inv_rms = lax.rsqrt(jnp.mean(inputs * inputs, axis=1, keepdims=True) + epsilon)
    scaled = inputs * inv_rms
    normed = (scaled * norm_gain[None, :]).astype(bf16)

    own_ids = lax.dynamic_slice_in_dim(route_ids, tp_index * tok_rows, tok_rows, 0)
    own_wts = lax.dynamic_slice_in_dim(route_wts, tp_index * tok_rows, tok_rows, 0)
    experts = jnp.arange(sp_count, dtype=jnp.int32)
    marks = [own_ids[:, k : k + 1] == experts[None, :] for k in range(top_count)]
    any_mark = sum(m.astype(bf16) for m in marks)
    index = jnp.arange(tok_rows, dtype=jnp.int32)
    before = (index[:, None] > index[None, :]).astype(bf16)
    ranks = dot(before, any_mark, 1, 0)
    places = [
        own_ids[:, k] * capacity
        + jnp.sum(jnp.where(marks[k], ranks, 0.0), axis=1).astype(jnp.int32)
        for k in range(top_count)
    ]
    slot_index = jnp.arange(slots, dtype=jnp.int32)
    picks = [slot_index[:, None] == places[k][None, :] for k in range(top_count)]
    select = sum(p.astype(bf16) for p in picks)
    slot_rows = dot(select, normed, 1, 0).astype(bf16)
    pieces = ring_gather(w_down)
    down_all = [w_down, *(jnp.concatenate(p, axis=0) for p in pieces[1:])]
    landed_rows = sent_over(slot_rows, sp_count)
    slot_wts = sum(
        jnp.sum(jnp.where(picks[k], own_wts[:, k][None, :], 0.0), axis=1, keepdims=True)
        for k in range(top_count)
    )
    slot_cot = (slot_wts * dot(select, stream_cot, 1, 0)).astype(bf16)
    slot_cot = packed(slot_cot, sp_count)
    landed_cot = exchange(slot_cot, SP).reshape(slots, model_width)
    own, left, right, far = ring_gather(landed_rows)
    rows = jnp.concatenate([own, *left, *right, *far], axis=0)

    far_h = dot(landed_cot, down_all[3], 1, 1).astype(bf16)
    left_h = dot(landed_cot, down_all[1], 1, 1).astype(bf16)
    right_h = dot(landed_cot, down_all[2], 1, 1).astype(bf16)
    own_h = dot(landed_cot, down_all[0], 1, 1)
    got = [shift(right_h, "tp", 1), shift(left_h, "tp", -1), shift(far_h, "tp", 2)]
    grad_hidden = jnp.concatenate([own_h, *(g.astype(f32) for g in got)], axis=0)
    gate_pre = dot(rows, w_gate, 1, 0)
    up_pre = dot(rows, w_up, 1, 0)
    gate_sig = jax.nn.sigmoid(gate_pre)
    gate_act = gate_pre * gate_sig
    hidden = (gate_act * up_pre).astype(bf16)
    gate_rate = up_pre * gate_sig * (1.0 + gate_pre * (1.0 - gate_sig))
    gate_act, gate_rate, hidden = lax.optimization_barrier((gate_act, gate_rate, hidden))
    up_grad = (grad_hidden * gate_act).astype(bf16)
    gate_grad = (grad_hidden * gate_rate).astype(bf16)

    returned = []
    for c in cols:
        back = (dot(gate_grad, w_gate[c], 1, 1) + dot(up_grad, w_up[c], 1, 1)).astype(bf16)
        back = [back[i * slots : (i + 1) * slots] for i in range(tp_count)]
        summed = ring_reduce(*back)
        returned.append(sent_over(summed, sp_count))
    cots = late_gather(landed_cot)
    gate_wgrad = dot(rows, gate_grad, 0, 0)
    up_wgrad = dot(rows, up_grad, 0, 0)
    down_grad = dot(hidden, cots, 0, 0)

    grad_normed = jnp.concatenate([dot(select, r, 0, 0) for r in returned], axis=1)
    q_term = grad_normed * norm_gain[None, :]
    stream_grad = (
        stream_cot.astype(f32)
        + inv_rms * (q_term - scaled * jnp.mean(q_term * scaled, axis=1, keepdims=True))
    ).astype(bf16)
    own, left, right, far = ring_gather(stream_grad)
    group_grad = jnp.concatenate([own, *right, *far, *left], axis=0)
    mix_turned = dot(group_grad, out_proj, 1, 1).astype(bf16)

    def turned(x, by):
        twice = jnp.concatenate([x, x], axis=0)
        return lax.dynamic_slice_in_dim(twice, by * tok_rows, tp_count * tok_rows, 0)

    grad_mix = turned(mix_turned, (tp_count - tp_index) % tp_count)

    rim_prev = from_behind(jnp.stack([conv_c[-2:], conv_h[-2:]]), SP, 1)
    gate_ext = jnp.concatenate([rim_prev[0], conv_c], axis=0).astype(f32)
    value_ext = jnp.concatenate([rim_prev[1], conv_h], axis=0).astype(f32)
    conv_in = gate_ext * value_ext
    conv_out = (
        conv_taps[0][None, :] * conv_in[:-2]
        + conv_taps[1][None, :] * conv_in[1:-1]
        + conv_taps[2][None, :] * conv_in[2:]
    )
    mixed = turned((conv_b.astype(f32) * conv_out).astype(bf16), tp_index)

    proj = dot(group_grad, mixed, 0, 0)
    nz, ny, nc = (lax.axis_size(a) for a in SP)
    own_depth = model_width // sp_count
    width = proj.shape[1]
    proj = proj.reshape(nz * ny, nc, own_depth, width).astype(bf16)
    proj = exchange(jnp.moveaxis(proj, 1, 0), "c")
    proj = proj.astype(f32).sum(axis=0).astype(bf16)
    proj_grad = exchange(proj, ("z", "y")).astype(f32).sum(axis=0)

    grad_b = (grad_mix.astype(f32) * conv_out).astype(bf16)
    rim_next = from_behind(jnp.stack([grad_mix[:2], conv_b[:2]]), SP, -1)
    conv_grad = grad_mix.astype(f32) * conv_b.astype(f32)
    next_grad = rim_next[0].astype(f32) * rim_next[1].astype(f32)
    grad_ext = jnp.concatenate([conv_grad, next_grad], axis=0)
    grad_in = (
        conv_taps[2][None, :] * grad_ext[:-2]
        + conv_taps[1][None, :] * grad_ext[1:-1]
        + conv_taps[0][None, :] * grad_ext[2:]
    )
    grad_c = (grad_in * conv_h.astype(f32)).astype(bf16)
    grad_h = (grad_in * conv_c.astype(f32)).astype(bf16)
    return (gate_wgrad[None], up_wgrad[None], down_grad[None], proj_grad, grad_b, grad_c, grad_h)


def solution(mesh):
    split = Mesh(mesh.devices.reshape(8, 4, 2, 4), (*SP, "tp"))
    in_specs = (
        P((*SP, "tp"), None),
        P((*SP, "tp"), None),
        P(SP, None),
        P(SP, None),
        P(),
        P(SP, None, "tp"),
        P(SP, None, "tp"),
        P(SP, "tp", None),
        P("tp", None),
        P(SP, "tp"),
        P(SP, "tp"),
        P(SP, "tp"),
        P(None, "tp"),
    )
    out_specs = (
        P(SP, None, "tp"),
        P(SP, None, "tp"),
        P(SP, "tp", None),
        P(SP, "tp"),
        P(SP, "tp"),
        P(SP, "tp"),
        P(SP, "tp"),
    )
    return jax.shard_map(step, mesh=split, in_specs=in_specs, out_specs=out_specs, check_vma=False)
```

```python
import jax
import jax.numpy as jnp
from jax import lax
from jax.sharding import Mesh, PartitionSpec as P


epsilon = 1e-06
SP = ("z", "y", "c")
bf16 = jnp.bfloat16
f32 = jnp.float32


def shift(x, axis, steps):
    count = lax.axis_size(axis)
    return lax.ppermute(x, axis, [(i, (i + steps) % count) for i in range(count)])


def from_behind(value, axis, steps):
    count = lax.axis_size(axis)
    initial, last = (max(0, -steps), min(count, count - steps))
    return lax.ppermute(value, axis, [(source, source + steps) for source in range(initial, last)])


def exchange(x, axis):
    return lax.all_to_all(x, axis, split_axis=0, concat_axis=0, tiled=True)


def ring_gather(x):
    half = x.shape[0] // 2
    a, b = x[:half], x[half:]
    left_a = shift(a, "tp", 1)
    right_b = shift(b, "tp", -1)
    left_b = shift(b, "tp", 1)
    right_a = shift(a, "tp", -1)
    far_a = shift(left_a, "tp", 1)
    far_b = shift(right_b, "tp", -1)
    return x, (left_a, left_b), (right_a, right_b), (far_a, far_b)


def late_gather(x):
    half = x.shape[0] // 2
    left = shift(x, "tp", 1)
    right = shift(x, "tp", -1)
    far_a = shift(left[:half], "tp", 1)
    far_b = shift(right[half:], "tp", -1)
    return x, left, right, jnp.concatenate([far_a, far_b], axis=0)


def ring_reduce(own, left, right, far):
    half = own.shape[0] // 2
    from_left = shift(far[:half], "tp", 1)
    from_right = shift(far[half:], "tp", -1)
    right_a = (right[:half].astype(f32) + from_left.astype(f32)).astype(bf16)
    left_b = (left[half:].astype(f32) + from_right.astype(f32)).astype(bf16)
    l_b = shift(right[half:], "tp", 1)
    r_a = shift(left[:half], "tp", -1)
    l_a = shift(right_a, "tp", 1)
    r_b = shift(left_b, "tp", -1)
    l_a, l_b, r_a, r_b = lax.optimization_barrier((l_a, l_b, r_a, r_b))
    top = own[:half].astype(f32) + l_a.astype(f32) + r_a.astype(f32)
    low = own[half:].astype(f32) + l_b.astype(f32) + r_b.astype(f32)
    return jnp.concatenate([top, low], axis=0).astype(bf16)


def dot(a, b, ca, cb):
    return lax.dot_general(a, b, (((ca,), (cb,)), ((), ())), preferred_element_type=f32)


def packed(x, sp_count):
    slots, width = x.shape
    return x.reshape(sp_count, slots // sp_count * (width // 128), 128)


def sent_over(x, sp_count):
    return exchange(packed(x, sp_count), SP).reshape(x.shape)


def step(
    stream_in,
    stream_cot,
    route_ids,
    route_wts,
    norm_gain,
    w_gate,
    w_up,
    w_down,
    out_proj,
    conv_b,
    conv_c,
    conv_h,
    conv_taps,
):
    tp_count = lax.axis_size("tp")
    sp_count = lax.axis_size(SP)
    tp_index = lax.axis_index("tp")
    tok_rows, model_width = stream_in.shape
    top_count = route_ids.shape[1]
    capacity = max(2, 5 * top_count * tok_rows // (4 * sp_count))
    slots = sp_count * capacity
    halves = 2
    part = model_width // halves
    cols = [slice(i * part, (i + 1) * part) for i in range(halves)]
    w_gate, w_up, w_down = w_gate[0], w_up[0], w_down[0]

    inputs = stream_in.astype(f32)
    inv_rms = lax.rsqrt(jnp.mean(inputs * inputs, axis=1, keepdims=True) + epsilon)
    scaled = inputs * inv_rms
    normed = (scaled * norm_gain[None, :]).astype(bf16)

    own_ids = lax.dynamic_slice_in_dim(route_ids, tp_index * tok_rows, tok_rows, 0)
    own_wts = lax.dynamic_slice_in_dim(route_wts, tp_index * tok_rows, tok_rows, 0)
    experts = jnp.arange(sp_count, dtype=jnp.int32)
    marks = [own_ids[:, k : k + 1] == experts[None, :] for k in range(top_count)]
    any_mark = sum(m.astype(bf16) for m in marks)
    index = jnp.arange(tok_rows, dtype=jnp.int32)
    before = (index[:, None] > index[None, :]).astype(bf16)
    ranks = dot(before, any_mark, 1, 0)
    places = [
        own_ids[:, k] * capacity
        + jnp.sum(jnp.where(marks[k], ranks, 0.0), axis=1).astype(jnp.int32)
        for k in range(top_count)
    ]
    slot_index = jnp.arange(slots, dtype=jnp.int32)
    picks = [slot_index[:, None] == places[k][None, :] for k in range(top_count)]
    select = sum(p.astype(bf16) for p in picks)
    def turned(x, by):
        twice = jnp.concatenate([x, x], axis=0)
        return lax.dynamic_slice_in_dim(twice, by * tok_rows, tp_count * tok_rows, 0)

    rim_prev = from_behind(jnp.stack([conv_c[-2:], conv_h[-2:]]), SP, 1)
    gate_ext = jnp.concatenate([rim_prev[0], conv_c], axis=0).astype(f32)
    value_ext = jnp.concatenate([rim_prev[1], conv_h], axis=0).astype(f32)
    conv_in = gate_ext * value_ext
    conv_out = (
        conv_taps[0][None, :] * conv_in[:-2]
        + conv_taps[1][None, :] * conv_in[1:-1]
        + conv_taps[2][None, :] * conv_in[2:]
    )
    mixed = turned((conv_b.astype(f32) * conv_out).astype(bf16), tp_index)

    slot_rows = dot(select, normed, 1, 0).astype(bf16)
    down_all = late_gather(w_down)
    landed_rows = sent_over(slot_rows, sp_count)
    slot_wts = sum(
        jnp.sum(jnp.where(picks[k], own_wts[:, k][None, :], 0.0), axis=1, keepdims=True)
        for k in range(top_count)
    )
    slot_cot = (slot_wts * dot(select, stream_cot, 1, 0)).astype(bf16)
    slot_cot = packed(slot_cot, sp_count)
    landed_cot = exchange(slot_cot, SP).reshape(slots, model_width)
    own, left, right, far = ring_gather(landed_rows)
    rows = jnp.concatenate([own, *left, *right, *far], axis=0)

    far_h = dot(landed_cot, down_all[3], 1, 1).astype(bf16)
    left_h = dot(landed_cot, down_all[1], 1, 1).astype(bf16)
    right_h = dot(landed_cot, down_all[2], 1, 1).astype(bf16)
    own_h = dot(landed_cot, down_all[0], 1, 1)
    got = [shift(right_h, "tp", 1), shift(left_h, "tp", -1), shift(far_h, "tp", 2)]
    grad_hidden = jnp.concatenate([own_h, *(g.astype(f32) for g in got)], axis=0)
    gate_pre = dot(rows, w_gate, 1, 0)
    up_pre = dot(rows, w_up, 1, 0)
    gate_sig = jax.nn.sigmoid(gate_pre)
    gate_act = gate_pre * gate_sig
    hidden = (gate_act * up_pre).astype(bf16)
    gate_rate = up_pre * gate_sig * (1.0 + gate_pre * (1.0 - gate_sig))
    gate_act, gate_rate, hidden, conv_out, mixed = lax.optimization_barrier(
        (gate_act, gate_rate, hidden, conv_out, mixed)
    )
    up_grad = (grad_hidden * gate_act).astype(bf16)
    gate_grad = (grad_hidden * gate_rate).astype(bf16)

    returned = []
    for c in cols:
        back = (dot(gate_grad, w_gate[c], 1, 1) + dot(up_grad, w_up[c], 1, 1)).astype(bf16)
        back = [back[i * slots : (i + 1) * slots] for i in range(tp_count)]
        summed = ring_reduce(*back)
        returned.append(sent_over(summed, sp_count))
    cots = late_gather(landed_cot)
    gate_wgrad = dot(rows, gate_grad, 0, 0)
    up_wgrad = dot(rows, up_grad, 0, 0)
    down_grad = sum(dot(hidden[i * slots : (i + 1) * slots], r, 0, 0) for i, r in enumerate(cots))

    grad_normed = jnp.concatenate([dot(select, r, 0, 0) for r in returned], axis=1)
    q_term = grad_normed * norm_gain[None, :]
    stream_grad = (
        stream_cot.astype(f32)
        + inv_rms * (q_term - scaled * jnp.mean(q_term * scaled, axis=1, keepdims=True))
    ).astype(bf16)
    own, left, right, far = ring_gather(stream_grad)
    group_grad = jnp.concatenate([own, *right, *far, *left], axis=0)
    mix_turned = dot(group_grad, out_proj, 1, 1).astype(bf16)

    grad_mix = turned(mix_turned, (tp_count - tp_index) % tp_count)

    proj = dot(group_grad, mixed, 0, 0)
    nz, ny, nc = (lax.axis_size(a) for a in SP)
    own_depth = model_width // sp_count
    width = proj.shape[1]
    proj = proj.reshape(nz * ny, nc, own_depth, width).astype(bf16)
    proj = exchange(jnp.moveaxis(proj, 1, 0), "c")
    proj = proj.astype(f32).sum(axis=0).astype(bf16)
    proj = exchange(proj, ("z", "y"))
    proj_grad = proj.astype(f32).sum(axis=0)

    grad_b = (grad_mix.astype(f32) * conv_out).astype(bf16)
    rim_next = from_behind(jnp.stack([grad_mix[:2], conv_b[:2]]), SP, -1)
    conv_grad = grad_mix.astype(f32) * conv_b.astype(f32)
    next_grad = rim_next[0].astype(f32) * rim_next[1].astype(f32)
    grad_ext = jnp.concatenate([conv_grad, next_grad], axis=0)
    grad_in = (
        conv_taps[2][None, :] * grad_ext[:-2]
        + conv_taps[1][None, :] * grad_ext[1:-1]
        + conv_taps[0][None, :] * grad_ext[2:]
    )
    grad_c = (grad_in * conv_h.astype(f32)).astype(bf16)
    grad_h = (grad_in * conv_c.astype(f32)).astype(bf16)
    return (gate_wgrad[None], up_wgrad[None], down_grad[None], proj_grad, grad_b, grad_c, grad_h)


def solution(mesh):
    split = Mesh(mesh.devices.reshape(8, 4, 2, 4), (*SP, "tp"))
    in_specs = (
        P((*SP, "tp"), None),
        P((*SP, "tp"), None),
        P(SP, None),
        P(SP, None),
        P(),
        P(SP, None, "tp"),
        P(SP, None, "tp"),
        P(SP, "tp", None),
        P("tp", None),
        P(SP, "tp"),
        P(SP, "tp"),
        P(SP, "tp"),
        P(None, "tp"),
    )
    out_specs = (
        P(SP, None, "tp"),
        P(SP, None, "tp"),
        P(SP, "tp", None),
        P(SP, "tp"),
        P(SP, "tp"),
        P(SP, "tp"),
        P(SP, "tp"),
    )
    return jax.shard_map(step, mesh=split, in_specs=in_specs, out_specs=out_specs, check_vma=False)
```

```python
import jax
import jax.numpy as jnp
from jax import lax
from jax.sharding import Mesh, PartitionSpec as P


epsilon = 1e-06
SP = ("z", "y", "c")
bf16 = jnp.bfloat16
f32 = jnp.float32


def shift(x, axis, steps):
    count = lax.axis_size(axis)
    return lax.ppermute(x, axis, [(i, (i + steps) % count) for i in range(count)])


def from_behind(value, axis, steps):
    count = lax.axis_size(axis)
    initial, last = (max(0, -steps), min(count, count - steps))
    return lax.ppermute(value, axis, [(source, source + steps) for source in range(initial, last)])


def exchange(x, axis):
    return lax.all_to_all(x, axis, split_axis=0, concat_axis=0, tiled=True)


def ring_gather(a, b):
    left_a = shift(a, "tp", 1)
    right_b = shift(b, "tp", -1)
    left_b = shift(b, "tp", 1)
    right_a = shift(a, "tp", -1)
    far_a = shift(left_a, "tp", 1)
    far_b = shift(right_b, "tp", -1)
    return (left_a, left_b), (right_a, right_b), (far_a, far_b)


def late_gather(x):
    half = x.shape[0] // 2
    left = shift(x, "tp", 1)
    right = shift(x, "tp", -1)
    far_a = shift(left[:half], "tp", 1)
    far_b = shift(right[half:], "tp", -1)
    return x, left, right, jnp.concatenate([far_a, far_b], axis=0)


def ring_reduce(own, left, right, far):
    half = own.shape[0] // 2
    from_left = shift(far[:half], "tp", 1)
    from_right = shift(far[half:], "tp", -1)
    right_a = (right[:half].astype(f32) + from_left.astype(f32)).astype(bf16)
    left_b = (left[half:].astype(f32) + from_right.astype(f32)).astype(bf16)
    l_b = shift(right[half:], "tp", 1)
    r_a = shift(left[:half], "tp", -1)
    l_a = shift(right_a, "tp", 1)
    r_b = shift(left_b, "tp", -1)
    l_a, l_b, r_a, r_b = lax.optimization_barrier((l_a, l_b, r_a, r_b))
    top = own[:half].astype(f32) + l_a.astype(f32) + r_a.astype(f32)
    low = own[half:].astype(f32) + l_b.astype(f32) + r_b.astype(f32)
    return jnp.concatenate([top, low], axis=0).astype(bf16)


def dot(a, b, ca, cb):
    return lax.dot_general(a, b, (((ca,), (cb,)), ((), ())), preferred_element_type=f32)


def packed(x, sp_count):
    slots, width = x.shape
    return x.reshape(sp_count, slots // sp_count * (width // 128), 128)


def sent_over(x, sp_count):
    return exchange(packed(x, sp_count), SP).reshape(x.shape)


def step(
    stream_in,
    stream_cot,
    route_ids,
    route_wts,
    norm_gain,
    w_gate,
    w_up,
    w_down,
    out_proj,
    conv_b,
    conv_c,
    conv_h,
    conv_taps,
):
    tp_count = lax.axis_size("tp")
    sp_count = lax.axis_size(SP)
    tp_index = lax.axis_index("tp")
    tok_rows, model_width = stream_in.shape
    top_count = route_ids.shape[1]
    capacity = max(2, 5 * top_count * tok_rows // (4 * sp_count))
    slots = sp_count * capacity
    halves = 2
    part = model_width // halves
    cols = [slice(i * part, (i + 1) * part) for i in range(halves)]
    w_gate, w_up, w_down = w_gate[0], w_up[0], w_down[0]

    inputs = stream_in.astype(f32)
    inv_rms = lax.rsqrt(jnp.mean(inputs * inputs, axis=1, keepdims=True) + epsilon)
    scaled = inputs * inv_rms
    normed = (scaled * norm_gain[None, :]).astype(bf16)

    own_ids = lax.dynamic_slice_in_dim(route_ids, tp_index * tok_rows, tok_rows, 0)
    own_wts = lax.dynamic_slice_in_dim(route_wts, tp_index * tok_rows, tok_rows, 0)
    experts = jnp.arange(sp_count, dtype=jnp.int32)
    marks = [own_ids[:, k : k + 1] == experts[None, :] for k in range(top_count)]
    any_mark = sum(m.astype(bf16) for m in marks)
    index = jnp.arange(tok_rows, dtype=jnp.int32)
    before = (index[:, None] > index[None, :]).astype(bf16)
    ranks = dot(before, any_mark, 1, 0)
    places = [
        own_ids[:, k] * capacity
        + jnp.sum(jnp.where(marks[k], ranks, 0.0), axis=1).astype(jnp.int32)
        for k in range(top_count)
    ]
    slot_index = jnp.arange(slots, dtype=jnp.int32)
    picks = [slot_index[:, None] == places[k][None, :] for k in range(top_count)]
    select = sum(p.astype(bf16) for p in picks)
    def turned(x, by):
        twice = jnp.concatenate([x, x], axis=0)
        return lax.dynamic_slice_in_dim(twice, by * tok_rows, tp_count * tok_rows, 0)

    rim_prev = from_behind(jnp.stack([conv_c[-2:], conv_h[-2:]]), SP, 1)
    gate_ext = jnp.concatenate([rim_prev[0], conv_c], axis=0).astype(f32)
    value_ext = jnp.concatenate([rim_prev[1], conv_h], axis=0).astype(f32)
    conv_in = gate_ext * value_ext
    conv_out = (
        conv_taps[0][None, :] * conv_in[:-2]
        + conv_taps[1][None, :] * conv_in[1:-1]
        + conv_taps[2][None, :] * conv_in[2:]
    )
    mixed = turned((conv_b.astype(f32) * conv_out).astype(bf16), tp_index)

    slot_rows = dot(select, normed, 1, 0).astype(bf16)
    down_all = jnp.concatenate(late_gather(w_down), axis=0)
    landed_rows = exchange(packed(slot_rows, sp_count), SP)
    slot_wts = sum(
        jnp.sum(jnp.where(picks[k], own_wts[:, k][None, :], 0.0), axis=1, keepdims=True)
        for k in range(top_count)
    )
    slot_cot = (slot_wts * dot(select, stream_cot, 1, 0)).astype(bf16)
    slot_cot = packed(slot_cot, sp_count)
    landed_cot = exchange(slot_cot, SP).reshape(slots, model_width)
    near = [x.reshape(-1, model_width) for x in jnp.split(landed_rows, 2)]
    left, right, far = ring_gather(*near)
    rows = jnp.concatenate([*near, *left, *right, *far], axis=0)

    mine = dot(landed_cot, down_all, 1, 1)
    units = w_down.shape[0]
    own_h, left_h, right_h, far_h = (
        mine[:, i * units : (i + 1) * units] for i in range(tp_count)
    )
    left_h, right_h, far_h = (x.astype(bf16) for x in (left_h, right_h, far_h))
    from_far = shift(far_h, "tp", 2)
    from_left, from_right = shift(right_h, "tp", 1), shift(left_h, "tp", -1)
    got = [from_left, from_right, from_far]
    grad_hidden = jnp.concatenate([own_h, *(g.astype(f32) for g in got)], axis=0)
    gate_pre = dot(rows, w_gate, 1, 0)
    up_pre = dot(rows, w_up, 1, 0)
    gate_sig = jax.nn.sigmoid(gate_pre)
    gate_act = gate_pre * gate_sig
    hidden = (gate_act * up_pre).astype(bf16)
    gate_rate = up_pre * gate_sig * (1.0 + gate_pre * (1.0 - gate_sig))
    gate_act, gate_rate, hidden, conv_out, mixed = lax.optimization_barrier(
        (gate_act, gate_rate, hidden, conv_out, mixed)
    )
    up_grad = (grad_hidden * gate_act).astype(bf16)
    gate_grad = (grad_hidden * gate_rate).astype(bf16)

    returned = []
    for c in cols:
        back = (dot(gate_grad, w_gate[c], 1, 1) + dot(up_grad, w_up[c], 1, 1)).astype(bf16)
        back = [back[i * slots : (i + 1) * slots] for i in range(tp_count)]
        summed = ring_reduce(*back)
        returned.append(sent_over(summed, sp_count))
    cots = late_gather(landed_cot)
    gate_wgrad = dot(rows, gate_grad, 0, 0)
    up_wgrad = dot(rows, up_grad, 0, 0)
    down_grad = sum(dot(hidden[i * slots : (i + 1) * slots], r, 0, 0) for i, r in enumerate(cots))

    grad_normed = jnp.concatenate([dot(select, r, 0, 0) for r in returned], axis=1)
    q_term = grad_normed * norm_gain[None, :]
    stream_grad = (
        stream_cot.astype(f32)
        + inv_rms * (q_term - scaled * jnp.mean(q_term * scaled, axis=1, keepdims=True))
    ).astype(bf16)
    left, right, far = ring_gather(*jnp.split(stream_grad, 2))
    group_grad = jnp.concatenate([stream_grad, *right, *far, *left], axis=0)
    mix_turned = dot(group_grad, out_proj, 1, 1).astype(bf16)

    grad_mix = turned(mix_turned, (tp_count - tp_index) % tp_count)

    proj = dot(group_grad, mixed, 0, 0)
    nz, ny, nc = (lax.axis_size(a) for a in SP)
    own_depth = model_width // sp_count
    width = proj.shape[1]
    proj = proj.reshape(nz * ny, nc, own_depth, width).astype(bf16)
    proj = exchange(jnp.moveaxis(proj, 1, 0), "c")
    proj = proj.astype(f32).sum(axis=0).astype(bf16)
    proj = exchange(proj, ("z", "y"))
    proj_grad = proj.astype(f32).sum(axis=0)

    grad_b = (grad_mix.astype(f32) * conv_out).astype(bf16)
    rim_next = from_behind(jnp.stack([grad_mix[:2], conv_b[:2]]), SP, -1)
    conv_grad = grad_mix.astype(f32) * conv_b.astype(f32)
    next_grad = rim_next[0].astype(f32) * rim_next[1].astype(f32)
    grad_ext = jnp.concatenate([conv_grad, next_grad], axis=0)
    grad_in = (
        conv_taps[2][None, :] * grad_ext[:-2]
        + conv_taps[1][None, :] * grad_ext[1:-1]
        + conv_taps[0][None, :] * grad_ext[2:]
    )
    grad_c = (grad_in * conv_h.astype(f32)).astype(bf16)
    grad_h = (grad_in * conv_c.astype(f32)).astype(bf16)
    return (gate_wgrad[None], up_wgrad[None], down_grad[None], proj_grad, grad_b, grad_c, grad_h)


def solution(mesh):
    split = Mesh(mesh.devices.reshape(8, 4, 2, 4), (*SP, "tp"))
    in_specs = (
        P((*SP, "tp"), None),
        P((*SP, "tp"), None),
        P(SP, None),
        P(SP, None),
        P(),
        P(SP, None, "tp"),
        P(SP, None, "tp"),
        P(SP, "tp", None),
        P("tp", None),
        P(SP, "tp"),
        P(SP, "tp"),
        P(SP, "tp"),
        P(None, "tp"),
    )
    out_specs = (
        P(SP, None, "tp"),
        P(SP, None, "tp"),
        P(SP, "tp", None),
        P(SP, "tp"),
        P(SP, "tp"),
        P(SP, "tp"),
        P(SP, "tp"),
    )
    return jax.shard_map(step, mesh=split, in_specs=in_specs, out_specs=out_specs, check_vma=False)
```

```python
import jax
import jax.numpy as jnp
from jax import lax
from jax.sharding import Mesh, PartitionSpec as P


epsilon = 1e-06
SP = ("z", "y", "c")
bf16 = jnp.bfloat16
f32 = jnp.float32


def shift(x, axis, steps):
    count = lax.axis_size(axis)
    return lax.ppermute(x, axis, [(i, (i + steps) % count) for i in range(count)])


def from_behind(value, axis, steps):
    count = lax.axis_size(axis)
    initial, last = (max(0, -steps), min(count, count - steps))
    return lax.ppermute(value, axis, [(source, source + steps) for source in range(initial, last)])


def exchange(x, axis):
    return lax.all_to_all(x, axis, split_axis=0, concat_axis=0, tiled=True)


def ring_gather(a, b):
    left_a = shift(a, "tp", 1)
    right_b = shift(b, "tp", -1)
    left_b = shift(b, "tp", 1)
    right_a = shift(a, "tp", -1)
    far_a = shift(left_a, "tp", 1)
    far_b = shift(right_b, "tp", -1)
    return (left_a, left_b), (right_a, right_b), (far_a, far_b)


def late_gather(x):
    half = x.shape[0] // 2
    left = shift(x, "tp", 1)
    right = shift(x, "tp", -1)
    far_a = shift(left[:half], "tp", 1)
    far_b = shift(right[half:], "tp", -1)
    return x, left, right, jnp.concatenate([far_a, far_b], axis=0)


def ring_reduce(own, left, right, far):
    half = own.shape[0] // 2
    from_left = shift(far[:half], "tp", 1)
    from_right = shift(far[half:], "tp", -1)
    right_a = (right[:half].astype(f32) + from_left.astype(f32)).astype(bf16)
    left_b = (left[half:].astype(f32) + from_right.astype(f32)).astype(bf16)
    l_b = shift(right[half:], "tp", 1)
    r_a = shift(left[:half], "tp", -1)
    l_a = shift(right_a, "tp", 1)
    r_b = shift(left_b, "tp", -1)
    l_a, l_b, r_a, r_b = lax.optimization_barrier((l_a, l_b, r_a, r_b))
    top = own[:half].astype(f32) + l_a.astype(f32) + r_a.astype(f32)
    low = own[half:].astype(f32) + l_b.astype(f32) + r_b.astype(f32)
    return jnp.concatenate([top, low], axis=0).astype(bf16)


def dot(a, b, ca, cb):
    return lax.dot_general(a, b, (((ca,), (cb,)), ((), ())), preferred_element_type=f32)


def packed(x, sp_count):
    slots, width = x.shape
    return x.reshape(sp_count, slots // sp_count * (width // 128), 128)


def sent_over(x, sp_count):
    return exchange(packed(x, sp_count), SP).reshape(x.shape)


def step(
    stream_in,
    stream_cot,
    route_ids,
    route_wts,
    norm_gain,
    w_gate,
    w_up,
    w_down,
    out_proj,
    conv_b,
    conv_c,
    conv_h,
    conv_taps,
):
    tp_count = lax.axis_size("tp")
    sp_count = lax.axis_size(SP)
    tp_index = lax.axis_index("tp")
    tok_rows, model_width = stream_in.shape
    top_count = route_ids.shape[1]
    capacity = max(2, 5 * top_count * tok_rows // (4 * sp_count))
    slots = sp_count * capacity
    halves = 2
    part = model_width // halves
    cols = [slice(i * part, (i + 1) * part) for i in range(halves)]
    w_gate, w_up, w_down = w_gate[0], w_up[0], w_down[0]

    inputs = stream_in.astype(f32)
    inv_rms = lax.rsqrt(jnp.mean(inputs * inputs, axis=1, keepdims=True) + epsilon)
    scaled = inputs * inv_rms
    normed = (scaled * norm_gain[None, :]).astype(bf16)

    own_ids = lax.dynamic_slice_in_dim(route_ids, tp_index * tok_rows, tok_rows, 0)
    own_wts = lax.dynamic_slice_in_dim(route_wts, tp_index * tok_rows, tok_rows, 0)
    experts = jnp.arange(sp_count, dtype=jnp.int32)
    marks = [own_ids[:, k : k + 1] == experts[None, :] for k in range(top_count)]
    any_mark = sum(m.astype(bf16) for m in marks)
    index = jnp.arange(tok_rows, dtype=jnp.int32)
    before = (index[:, None] > index[None, :]).astype(bf16)
    ranks = dot(before, any_mark, 1, 0)
    places = [
        own_ids[:, k] * capacity
        + jnp.sum(jnp.where(marks[k], ranks, 0.0), axis=1).astype(jnp.int32)
        for k in range(top_count)
    ]
    slot_index = jnp.arange(slots, dtype=jnp.int32)
    picks = [slot_index[:, None] == places[k][None, :] for k in range(top_count)]
    select = sum(p.astype(bf16) for p in picks)
    def turned(x, by):
        twice = jnp.concatenate([x, x], axis=0)
        return lax.dynamic_slice_in_dim(twice, by * tok_rows, tp_count * tok_rows, 0)

    rim_prev = from_behind(jnp.stack([conv_c[-2:], conv_h[-2:]]), SP, 1)
    gate_ext = jnp.concatenate([rim_prev[0], conv_c], axis=0).astype(f32)
    value_ext = jnp.concatenate([rim_prev[1], conv_h], axis=0).astype(f32)
    conv_in = gate_ext * value_ext
    conv_out = (
        conv_taps[0][None, :] * conv_in[:-2]
        + conv_taps[1][None, :] * conv_in[1:-1]
        + conv_taps[2][None, :] * conv_in[2:]
    )
    mixed = turned((conv_b.astype(f32) * conv_out).astype(bf16), tp_index)

    slot_rows = dot(select, normed, 1, 0).astype(bf16)
    down_all = late_gather(w_down)
    landed_rows = exchange(packed(slot_rows, sp_count), SP)
    slot_wts = sum(
        jnp.sum(jnp.where(picks[k], own_wts[:, k][None, :], 0.0), axis=1, keepdims=True)
        for k in range(top_count)
    )
    slot_cot = (slot_wts * dot(select, stream_cot, 1, 0)).astype(bf16)
    slot_cot = packed(slot_cot, sp_count)
    landed_cot = exchange(slot_cot, SP).reshape(slots, model_width)
    near = [x.reshape(-1, model_width) for x in jnp.split(landed_rows, 2)]
    left, right, far = ring_gather(*near)
    rows = jnp.concatenate([*near, *left, *right, *far], axis=0)

    own_h = dot(landed_cot, down_all[0], 1, 1)
    left_h, right_h, far_h = (dot(landed_cot, w, 1, 1).astype(bf16) for w in down_all[1:])
    from_far = shift(far_h, "tp", 2)
    from_left, from_right = shift(right_h, "tp", 1), shift(left_h, "tp", -1)
    got = [from_left, from_right, from_far]
    grad_hidden = jnp.concatenate([own_h, *(g.astype(f32) for g in got)], axis=0)
    gate_pre = dot(rows, w_gate, 1, 0)
    up_pre = dot(rows, w_up, 1, 0)
    gate_sig = jax.nn.sigmoid(gate_pre)
    gate_act = gate_pre * gate_sig
    hidden = (gate_act * up_pre).astype(bf16)
    gate_rate = up_pre * gate_sig * (1.0 + gate_pre * (1.0 - gate_sig))
    gate_act, gate_rate, hidden, conv_out, mixed = lax.optimization_barrier(
        (gate_act, gate_rate, hidden, conv_out, mixed)
    )
    up_grad = (grad_hidden * gate_act).astype(bf16)
    gate_grad = (grad_hidden * gate_rate).astype(bf16)

    returned = []
    for c in cols:
        back = (dot(gate_grad, w_gate[c], 1, 1) + dot(up_grad, w_up[c], 1, 1)).astype(bf16)
        back = [back[i * slots : (i + 1) * slots] for i in range(tp_count)]
        summed = ring_reduce(*back)
        returned.append(sent_over(summed, sp_count))
    cots = late_gather(landed_cot)
    gate_wgrad = dot(rows, gate_grad, 0, 0)
    up_wgrad = dot(rows, up_grad, 0, 0)
    down_grad = sum(dot(hidden[i * slots : (i + 1) * slots], r, 0, 0) for i, r in enumerate(cots))

    grad_normed = jnp.concatenate([dot(select, r, 0, 0) for r in returned], axis=1)
    q_term = grad_normed * norm_gain[None, :]
    stream_grad = (
        stream_cot.astype(f32)
        + inv_rms * (q_term - scaled * jnp.mean(q_term * scaled, axis=1, keepdims=True))
    ).astype(bf16)
    left, right, far = ring_gather(*jnp.split(stream_grad, 2))
    group_grad = jnp.concatenate([stream_grad, *right, *far, *left], axis=0)
    mix_turned = dot(group_grad, out_proj, 1, 1).astype(bf16)

    grad_mix = turned(mix_turned, (tp_count - tp_index) % tp_count)

    proj = dot(group_grad, mixed, 0, 0)
    nz, ny, nc = (lax.axis_size(a) for a in SP)
    own_depth = model_width // sp_count
    width = proj.shape[1]
    proj = proj.reshape(nz * ny, nc, own_depth, width).astype(bf16)
    proj = exchange(jnp.moveaxis(proj, 1, 0), "c")
    proj = proj.astype(f32).sum(axis=0).astype(bf16)
    proj = exchange(proj, ("z", "y"))
    proj_grad = proj.astype(f32).sum(axis=0)

    grad_b = (grad_mix.astype(f32) * conv_out).astype(bf16)
    rim_next = from_behind(jnp.stack([grad_mix[:2], conv_b[:2]]), SP, -1)
    conv_grad = grad_mix.astype(f32) * conv_b.astype(f32)
    next_grad = rim_next[0].astype(f32) * rim_next[1].astype(f32)
    grad_ext = jnp.concatenate([conv_grad, next_grad], axis=0)
    grad_in = (
        conv_taps[2][None, :] * grad_ext[:-2]
        + conv_taps[1][None, :] * grad_ext[1:-1]
        + conv_taps[0][None, :] * grad_ext[2:]
    )
    grad_c = (grad_in * conv_h.astype(f32)).astype(bf16)
    grad_h = (grad_in * conv_c.astype(f32)).astype(bf16)
    return (gate_wgrad[None], up_wgrad[None], down_grad[None], proj_grad, grad_b, grad_c, grad_h)


def solution(mesh):
    split = Mesh(mesh.devices.reshape(8, 4, 2, 4), (*SP, "tp"))
    in_specs = (
        P((*SP, "tp"), None),
        P((*SP, "tp"), None),
        P(SP, None),
        P(SP, None),
        P(),
        P(SP, None, "tp"),
        P(SP, None, "tp"),
        P(SP, "tp", None),
        P("tp", None),
        P(SP, "tp"),
        P(SP, "tp"),
        P(SP, "tp"),
        P(None, "tp"),
    )
    out_specs = (
        P(SP, None, "tp"),
        P(SP, None, "tp"),
        P(SP, "tp", None),
        P(SP, "tp"),
        P(SP, "tp"),
        P(SP, "tp"),
        P(SP, "tp"),
    )
    return jax.shard_map(step, mesh=split, in_specs=in_specs, out_specs=out_specs, check_vma=False)
```

```python
import jax
import jax.numpy as jnp
from jax import lax
from jax.sharding import Mesh, PartitionSpec as P


epsilon = 1e-06
SP = ("z", "y", "c")
bf16 = jnp.bfloat16
f32 = jnp.float32


def shift(x, axis, steps):
    count = lax.axis_size(axis)
    return lax.ppermute(x, axis, [(i, (i + steps) % count) for i in range(count)])


def from_behind(value, axis, steps):
    count = lax.axis_size(axis)
    initial, last = (max(0, -steps), min(count, count - steps))
    return lax.ppermute(value, axis, [(source, source + steps) for source in range(initial, last)])


def exchange(x, axis):
    return lax.all_to_all(x, axis, split_axis=0, concat_axis=0, tiled=True)


def ring_gather(a, b):
    left_a = shift(a, "tp", 1)
    right_b = shift(b, "tp", -1)
    left_b = shift(b, "tp", 1)
    right_a = shift(a, "tp", -1)
    far_a = shift(left_a, "tp", 1)
    far_b = shift(right_b, "tp", -1)
    return (left_a, left_b), (right_a, right_b), (far_a, far_b)


def late_gather(x):
    half = x.shape[0] // 2
    left = shift(x, "tp", 1)
    right = shift(x, "tp", -1)
    far_a = shift(left[:half], "tp", 1)
    far_b = shift(right[half:], "tp", -1)
    return x, left, right, jnp.concatenate([far_a, far_b], axis=0)


def ring_reduce(own, left_a, right_b, left_b, right_a, far_a, far_b):
    from_left = shift(far_a, "tp", 1)
    from_right = shift(far_b, "tp", -1)
    l_b = shift(right_b, "tp", 1)
    r_a = shift(left_a, "tp", -1)
    right_a = (right_a.astype(f32) + from_left.astype(f32)).astype(bf16)
    left_b = (left_b.astype(f32) + from_right.astype(f32)).astype(bf16)
    l_a = shift(right_a, "tp", 1)
    r_b = shift(left_b, "tp", -1)
    l_a, l_b, r_a, r_b = lax.optimization_barrier((l_a, l_b, r_a, r_b))
    half = own.shape[0] // 2
    top = own[:half].astype(f32) + l_a.astype(f32) + r_a.astype(f32)
    low = own[half:].astype(f32) + l_b.astype(f32) + r_b.astype(f32)
    return jnp.concatenate([top, low], axis=0).astype(bf16)


def dot(a, b, ca, cb):
    return lax.dot_general(a, b, (((ca,), (cb,)), ((), ())), preferred_element_type=f32)


def packed(x, sp_count):
    slots, width = x.shape
    return x.reshape(sp_count, slots // sp_count * (width // 128), 128)


def sent_over(x, sp_count):
    return exchange(packed(x, sp_count), SP).reshape(x.shape)


def step(
    stream_in,
    stream_cot,
    route_ids,
    route_wts,
    norm_gain,
    w_gate,
    w_up,
    w_down,
    out_proj,
    conv_b,
    conv_c,
    conv_h,
    conv_taps,
):
    tp_count = lax.axis_size("tp")
    sp_count = lax.axis_size(SP)
    tp_index = lax.axis_index("tp")
    tok_rows, model_width = stream_in.shape
    top_count = route_ids.shape[1]
    capacity = max(2, 5 * top_count * tok_rows // (4 * sp_count))
    slots = sp_count * capacity
    halves = 2
    part = model_width // halves
    cols = [slice(i * part, (i + 1) * part) for i in range(halves)]
    w_gate, w_up, w_down = w_gate[0], w_up[0], w_down[0]

    inputs = stream_in.astype(f32)
    inv_rms = lax.rsqrt(jnp.mean(inputs * inputs, axis=1, keepdims=True) + epsilon)
    scaled = inputs * inv_rms
    normed = (scaled * norm_gain[None, :]).astype(bf16)

    own_ids = lax.dynamic_slice_in_dim(route_ids, tp_index * tok_rows, tok_rows, 0)
    own_wts = lax.dynamic_slice_in_dim(route_wts, tp_index * tok_rows, tok_rows, 0)
    experts = jnp.arange(sp_count, dtype=jnp.int32)
    marks = [own_ids[:, k : k + 1] == experts[None, :] for k in range(top_count)]
    any_mark = sum(m.astype(bf16) for m in marks)
    index = jnp.arange(tok_rows, dtype=jnp.int32)
    before = (index[:, None] > index[None, :]).astype(bf16)
    ranks = dot(before, any_mark, 1, 0)
    places = [
        own_ids[:, k] * capacity
        + jnp.sum(jnp.where(marks[k], ranks, 0.0), axis=1).astype(jnp.int32)
        for k in range(top_count)
    ]
    slot_index = jnp.arange(slots, dtype=jnp.int32)
    picks = [slot_index[:, None] == places[k][None, :] for k in range(top_count)]
    select = sum(p.astype(bf16) for p in picks)
    def turned(x, by):
        twice = jnp.concatenate([x, x], axis=0)
        return lax.dynamic_slice_in_dim(twice, by * tok_rows, tp_count * tok_rows, 0)

    rim_prev = from_behind(jnp.stack([conv_c[-2:], conv_h[-2:]]), SP, 1)
    gate_ext = jnp.concatenate([rim_prev[0], conv_c], axis=0).astype(f32)
    value_ext = jnp.concatenate([rim_prev[1], conv_h], axis=0).astype(f32)
    conv_in = gate_ext * value_ext
    conv_out = (
        conv_taps[0][None, :] * conv_in[:-2]
        + conv_taps[1][None, :] * conv_in[1:-1]
        + conv_taps[2][None, :] * conv_in[2:]
    )
    mixed = turned((conv_b.astype(f32) * conv_out).astype(bf16), tp_index)

    slot_rows = dot(select, normed, 1, 0).astype(bf16)
    down_all = late_gather(w_down)
    landed_rows = exchange(packed(slot_rows, sp_count), SP)
    slot_wts = sum(
        jnp.sum(jnp.where(picks[k], own_wts[:, k][None, :], 0.0), axis=1, keepdims=True)
        for k in range(top_count)
    )
    slot_cot = (slot_wts * dot(select, stream_cot, 1, 0)).astype(bf16)
    slot_cot = packed(slot_cot, sp_count)
    landed_cot = exchange(slot_cot, SP).reshape(slots, model_width)
    near = [x.reshape(-1, model_width) for x in jnp.split(landed_rows, 2)]
    left, right, far = ring_gather(*near)
    rows = [
        jnp.concatenate([*near, left[0], right[1]], axis=0),
        jnp.concatenate([left[1], right[0], *far], axis=0),
    ]

    own_h = dot(landed_cot, down_all[0], 1, 1)
    left_h, right_h, far_h = (dot(landed_cot, w, 1, 1).astype(bf16) for w in down_all[1:])
    from_far = shift(far_h, "tp", 2)
    from_left, from_right = shift(right_h, "tp", 1), shift(left_h, "tp", -1)
    half = slots // 2
    grad_hidden = [
        jnp.concatenate(
            [own_h, from_left[:half].astype(f32), from_right[half:].astype(f32)], axis=0
        ),
        jnp.concatenate([from_left[half:], from_right[:half], from_far], axis=0).astype(f32),
    ]
    acts = []
    for i, r in enumerate(rows):
        gate_pre = dot(r, w_gate, 1, 0)
        up_pre = dot(r, w_up, 1, 0)
        gate_sig = jax.nn.sigmoid(gate_pre)
        gate_act = gate_pre * gate_sig
        hidden = (gate_act * up_pre).astype(bf16)
        gate_rate = up_pre * gate_sig * (1.0 + gate_pre * (1.0 - gate_sig))
        if i == 0:
            gate_act, gate_rate, hidden, conv_out, mixed = lax.optimization_barrier(
                (gate_act, gate_rate, hidden, conv_out, mixed)
            )
        else:
            gate_act, gate_rate, hidden = lax.optimization_barrier((gate_act, gate_rate, hidden))
        acts.append((gate_act, gate_rate, hidden))
    up_grad = [(g * a[0]).astype(bf16) for g, a in zip(grad_hidden, acts)]
    gate_grad = [(g * a[1]).astype(bf16) for g, a in zip(grad_hidden, acts)]

    returned = []
    for c in cols:
        direct, relayed = (
            (dot(gg, w_gate[c], 1, 1) + dot(ug, w_up[c], 1, 1)).astype(bf16)
            for gg, ug in zip(gate_grad, up_grad)
        )
        summed = ring_reduce(direct[:slots], *jnp.split(direct[slots:], 2), *jnp.split(relayed, 4))
        returned.append(sent_over(summed, sp_count))
    cots = late_gather(landed_cot)
    gate_wgrad = sum(dot(r, g, 0, 0) for r, g in zip(rows, gate_grad))
    up_wgrad = sum(dot(r, g, 0, 0) for r, g in zip(rows, up_grad))
    hid_1, hid_2 = acts[0][2], acts[1][2]
    hidden = [
        hid_1[:slots],
        jnp.concatenate([hid_1[slots : slots + half], hid_2[:half]], axis=0),
        jnp.concatenate([hid_2[half:slots], hid_1[slots + half :]], axis=0),
        hid_2[slots:],
    ]
    down_grad = sum(dot(h, r, 0, 0) for h, r in zip(hidden, cots))

    grad_normed = jnp.concatenate([dot(select, r, 0, 0) for r in returned], axis=1)
    q_term = grad_normed * norm_gain[None, :]
    stream_grad = (
        stream_cot.astype(f32)
        + inv_rms * (q_term - scaled * jnp.mean(q_term * scaled, axis=1, keepdims=True))
    ).astype(bf16)
    left, right, far = ring_gather(*jnp.split(stream_grad, 2))
    group_grad = jnp.concatenate([stream_grad, *right, *far, *left], axis=0)
    mix_turned = dot(group_grad, out_proj, 1, 1).astype(bf16)

    grad_mix = turned(mix_turned, (tp_count - tp_index) % tp_count)

    proj = dot(group_grad, mixed, 0, 0)
    nz, ny, nc = (lax.axis_size(a) for a in SP)
    own_depth = model_width // sp_count
    width = proj.shape[1]
    proj = proj.reshape(nz * ny, nc, own_depth, width).astype(bf16)
    proj = exchange(jnp.moveaxis(proj, 1, 0), "c")
    proj = proj.astype(f32).sum(axis=0).astype(bf16)
    proj = exchange(proj, ("z", "y"))
    proj_grad = proj.astype(f32).sum(axis=0)

    grad_b = (grad_mix.astype(f32) * conv_out).astype(bf16)
    rim_next = from_behind(jnp.stack([grad_mix[:2], conv_b[:2]]), SP, -1)
    conv_grad = grad_mix.astype(f32) * conv_b.astype(f32)
    next_grad = rim_next[0].astype(f32) * rim_next[1].astype(f32)
    grad_ext = jnp.concatenate([conv_grad, next_grad], axis=0)
    grad_in = (
        conv_taps[2][None, :] * grad_ext[:-2]
        + conv_taps[1][None, :] * grad_ext[1:-1]
        + conv_taps[0][None, :] * grad_ext[2:]
    )
    grad_c = (grad_in * conv_h.astype(f32)).astype(bf16)
    grad_h = (grad_in * conv_c.astype(f32)).astype(bf16)
    return (gate_wgrad[None], up_wgrad[None], down_grad[None], proj_grad, grad_b, grad_c, grad_h)


def solution(mesh):
    split = Mesh(mesh.devices.reshape(8, 4, 2, 4), (*SP, "tp"))
    in_specs = (
        P((*SP, "tp"), None),
        P((*SP, "tp"), None),
        P(SP, None),
        P(SP, None),
        P(),
        P(SP, None, "tp"),
        P(SP, None, "tp"),
        P(SP, "tp", None),
        P("tp", None),
        P(SP, "tp"),
        P(SP, "tp"),
        P(SP, "tp"),
        P(None, "tp"),
    )
    out_specs = (
        P(SP, None, "tp"),
        P(SP, None, "tp"),
        P(SP, "tp", None),
        P(SP, "tp"),
        P(SP, "tp"),
        P(SP, "tp"),
        P(SP, "tp"),
    )
    return jax.shard_map(step, mesh=split, in_specs=in_specs, out_specs=out_specs, check_vma=False)
```

```python
import jax
import jax.numpy as jnp
from jax import lax
from jax.sharding import Mesh, PartitionSpec as P


epsilon = 1e-06
SP = ("z", "y", "c")
bf16 = jnp.bfloat16
f32 = jnp.float32


def shift(x, axis, steps):
    count = lax.axis_size(axis)
    return lax.ppermute(x, axis, [(i, (i + steps) % count) for i in range(count)])


def from_behind(value, axis, steps):
    count = lax.axis_size(axis)
    initial, last = (max(0, -steps), min(count, count - steps))
    return lax.ppermute(value, axis, [(source, source + steps) for source in range(initial, last)])


def exchange(x, axis):
    return lax.all_to_all(x, axis, split_axis=0, concat_axis=0, tiled=True)


def ring_gather(a, b):
    left_a = shift(a, "tp", 1)
    right_b = shift(b, "tp", -1)
    left_b = shift(b, "tp", 1)
    right_a = shift(a, "tp", -1)
    far_a = shift(left_a, "tp", 1)
    far_b = shift(right_b, "tp", -1)
    return (left_a, left_b), (right_a, right_b), (far_a, far_b)


def late_gather(x):
    half = x.shape[0] // 2
    left = shift(x, "tp", 1)
    right = shift(x, "tp", -1)
    far_a = shift(left[:half], "tp", 1)
    far_b = shift(right[half:], "tp", -1)
    return x, left, right, jnp.concatenate([far_a, far_b], axis=0)


def ring_reduce(own, left_a, right_b, left_b, right_a, far_a, far_b):
    from_left = shift(far_a, "tp", 1)
    from_right = shift(far_b, "tp", -1)
    l_b = shift(right_b, "tp", 1)
    r_a = shift(left_a, "tp", -1)
    right_a = (right_a.astype(f32) + from_left.astype(f32)).astype(bf16)
    left_b = (left_b.astype(f32) + from_right.astype(f32)).astype(bf16)
    l_a = shift(right_a, "tp", 1)
    r_b = shift(left_b, "tp", -1)
    l_a, l_b, r_a, r_b = lax.optimization_barrier((l_a, l_b, r_a, r_b))
    half = own.shape[0] // 2
    top = own[:half].astype(f32) + l_a.astype(f32) + r_a.astype(f32)
    low = own[half:].astype(f32) + l_b.astype(f32) + r_b.astype(f32)
    return jnp.concatenate([top, low], axis=0).astype(bf16)


def dot(a, b, ca, cb):
    return lax.dot_general(a, b, (((ca,), (cb,)), ((), ())), preferred_element_type=f32)


def packed(x, sp_count):
    slots, width = x.shape
    return x.reshape(sp_count, slots // sp_count * (width // 128), 128)


def sent_over(x, sp_count):
    return exchange(packed(x, sp_count), SP).reshape(x.shape)


def step(
    stream_in,
    stream_cot,
    route_ids,
    route_wts,
    norm_gain,
    w_gate,
    w_up,
    w_down,
    out_proj,
    conv_b,
    conv_c,
    conv_h,
    conv_taps,
):
    tp_count = lax.axis_size("tp")
    sp_count = lax.axis_size(SP)
    tp_index = lax.axis_index("tp")
    tok_rows, model_width = stream_in.shape
    top_count = route_ids.shape[1]
    capacity = max(2, 5 * top_count * tok_rows // (4 * sp_count))
    slots = sp_count * capacity
    halves = 2
    part = model_width // halves
    cols = [slice(i * part, (i + 1) * part) for i in range(halves)]
    w_gate, w_up, w_down = w_gate[0], w_up[0], w_down[0]

    inputs = stream_in.astype(f32)
    inv_rms = lax.rsqrt(jnp.mean(inputs * inputs, axis=1, keepdims=True) + epsilon)
    scaled = inputs * inv_rms
    normed = (scaled * norm_gain[None, :]).astype(bf16)

    own_ids = lax.dynamic_slice_in_dim(route_ids, tp_index * tok_rows, tok_rows, 0)
    own_wts = lax.dynamic_slice_in_dim(route_wts, tp_index * tok_rows, tok_rows, 0)
    experts = jnp.arange(sp_count, dtype=jnp.int32)
    marks = [own_ids[:, k : k + 1] == experts[None, :] for k in range(top_count)]
    any_mark = sum(m.astype(bf16) for m in marks)
    index = jnp.arange(tok_rows, dtype=jnp.int32)
    before = (index[:, None] > index[None, :]).astype(bf16)
    ranks = dot(before, any_mark, 1, 0)
    places = [
        own_ids[:, k] * capacity
        + jnp.sum(jnp.where(marks[k], ranks, 0.0), axis=1).astype(jnp.int32)
        for k in range(top_count)
    ]
    slot_index = jnp.arange(slots, dtype=jnp.int32)
    picks = [slot_index[:, None] == places[k][None, :] for k in range(top_count)]
    select = sum(p.astype(bf16) for p in picks)
    def turned(x, by):
        twice = jnp.concatenate([x, x], axis=0)
        return lax.dynamic_slice_in_dim(twice, by * tok_rows, tp_count * tok_rows, 0)

    rim_prev = from_behind(jnp.stack([conv_c[-2:], conv_h[-2:]]), SP, 1)
    gate_ext = jnp.concatenate([rim_prev[0], conv_c], axis=0).astype(f32)
    value_ext = jnp.concatenate([rim_prev[1], conv_h], axis=0).astype(f32)
    conv_in = gate_ext * value_ext
    conv_out = (
        conv_taps[0][None, :] * conv_in[:-2]
        + conv_taps[1][None, :] * conv_in[1:-1]
        + conv_taps[2][None, :] * conv_in[2:]
    )
    mixed = turned((conv_b.astype(f32) * conv_out).astype(bf16), tp_index)

    slot_rows = dot(select, normed, 1, 0).astype(bf16)
    down_all = late_gather(w_down)
    landed_rows = exchange(packed(slot_rows, sp_count), SP)
    slot_wts = sum(
        jnp.sum(jnp.where(picks[k], own_wts[:, k][None, :], 0.0), axis=1, keepdims=True)
        for k in range(top_count)
    )
    slot_cot = (slot_wts * dot(select, stream_cot, 1, 0)).astype(bf16)
    slot_cot = packed(slot_cot, sp_count)
    landed_cot = exchange(slot_cot, SP).reshape(slots, model_width)
    near = [x.reshape(-1, model_width) for x in jnp.split(landed_rows, 2)]
    left, right, far = ring_gather(*near)
    rows = [
        jnp.concatenate(lax.optimization_barrier((*near, left[0], right[1])), axis=0),
        jnp.concatenate([left[1], right[0]], axis=0),
        jnp.concatenate(far, axis=0),
    ]

    left_h, right_h, far_h = (dot(landed_cot, w, 1, 1).astype(bf16) for w in down_all[1:])
    own_h = dot(landed_cot, down_all[0], 1, 1)
    from_far = shift(far_h, "tp", 2)
    from_left, from_right = shift(right_h, "tp", 1), shift(left_h, "tp", -1)
    half = slots // 2
    grad_hidden = [
        jnp.concatenate(
            [own_h, from_left[:half].astype(f32), from_right[half:].astype(f32)], axis=0
        ),
        jnp.concatenate([from_left[half:], from_right[:half]], axis=0).astype(f32),
        from_far.astype(f32),
    ]
    acts = []
    for i, r in enumerate(rows):
        gate_pre = dot(r, w_gate, 1, 0)
        up_pre = dot(r, w_up, 1, 0)
        gate_sig = jax.nn.sigmoid(gate_pre)
        gate_act = gate_pre * gate_sig
        hidden = (gate_act * up_pre).astype(bf16)
        gate_rate = up_pre * gate_sig * (1.0 + gate_pre * (1.0 - gate_sig))
        if i == 0:
            gate_act, gate_rate, hidden, conv_out, mixed = lax.optimization_barrier(
                (gate_act, gate_rate, hidden, conv_out, mixed)
            )
        else:
            gate_act, gate_rate, hidden = lax.optimization_barrier((gate_act, gate_rate, hidden))
        acts.append((gate_act, gate_rate, hidden))
    up_grad = [(g * a[0]).astype(bf16) for g, a in zip(grad_hidden, acts)]
    gate_grad = [(g * a[1]).astype(bf16) for g, a in zip(grad_hidden, acts)]

    returned = []
    for c in cols:
        direct, middle, relayed = (
            (dot(gg, w_gate[c], 1, 1) + dot(ug, w_up[c], 1, 1)).astype(bf16)
            for gg, ug in zip(gate_grad, up_grad)
        )
        summed = ring_reduce(
            direct[:slots], *jnp.split(direct[slots:], 2), *jnp.split(middle, 2), *jnp.split(relayed, 2)
        )
        returned.append(sent_over(summed, sp_count))
    cots = late_gather(landed_cot)
    gate_wgrad = sum(dot(r, g, 0, 0) for r, g in zip(rows, gate_grad))
    up_wgrad = sum(dot(r, g, 0, 0) for r, g in zip(rows, up_grad))
    hid_1, hid_2, hid_3 = (a[2] for a in acts)
    hidden = [
        hid_1[:slots],
        jnp.concatenate([hid_1[slots : slots + half], hid_2[:half]], axis=0),
        jnp.concatenate([hid_2[half:], hid_1[slots + half :]], axis=0),
        hid_3,
    ]
    down_grad = sum(dot(h, r, 0, 0) for h, r in zip(hidden, cots))

    grad_normed = jnp.concatenate([dot(select, r, 0, 0) for r in returned], axis=1)
    q_term = grad_normed * norm_gain[None, :]
    stream_grad = (
        stream_cot.astype(f32)
        + inv_rms * (q_term - scaled * jnp.mean(q_term * scaled, axis=1, keepdims=True))
    ).astype(bf16)
    left, right, far = ring_gather(*jnp.split(stream_grad, 2))
    group_grad = jnp.concatenate([stream_grad, *right, *far, *left], axis=0)
    mix_turned = dot(group_grad, out_proj, 1, 1).astype(bf16)

    grad_mix = turned(mix_turned, (tp_count - tp_index) % tp_count)

    proj = dot(group_grad, mixed, 0, 0)
    nz, ny, nc = (lax.axis_size(a) for a in SP)
    own_depth = model_width // sp_count
    width = proj.shape[1]
    proj = proj.reshape(nz * ny, nc, own_depth, width).astype(bf16)
    proj = exchange(jnp.moveaxis(proj, 1, 0), "c")
    proj = proj.astype(f32).sum(axis=0).astype(bf16)
    proj = exchange(proj, ("z", "y"))
    proj_grad = proj.astype(f32).sum(axis=0)

    grad_b = (grad_mix.astype(f32) * conv_out).astype(bf16)
    rim_next = from_behind(jnp.stack([grad_mix[:2], conv_b[:2]]), SP, -1)
    conv_grad = grad_mix.astype(f32) * conv_b.astype(f32)
    next_grad = rim_next[0].astype(f32) * rim_next[1].astype(f32)
    grad_ext = jnp.concatenate([conv_grad, next_grad], axis=0)
    grad_in = (
        conv_taps[2][None, :] * grad_ext[:-2]
        + conv_taps[1][None, :] * grad_ext[1:-1]
        + conv_taps[0][None, :] * grad_ext[2:]
    )
    grad_c = (grad_in * conv_h.astype(f32)).astype(bf16)
    grad_h = (grad_in * conv_c.astype(f32)).astype(bf16)
    return (gate_wgrad[None], up_wgrad[None], down_grad[None], proj_grad, grad_b, grad_c, grad_h)


def solution(mesh):
    split = Mesh(mesh.devices.reshape(8, 4, 2, 4), (*SP, "tp"))
    in_specs = (
        P((*SP, "tp"), None),
        P((*SP, "tp"), None),
        P(SP, None),
        P(SP, None),
        P(),
        P(SP, None, "tp"),
        P(SP, None, "tp"),
        P(SP, "tp", None),
        P("tp", None),
        P(SP, "tp"),
        P(SP, "tp"),
        P(SP, "tp"),
        P(None, "tp"),
    )
    out_specs = (
        P(SP, None, "tp"),
        P(SP, None, "tp"),
        P(SP, "tp", None),
        P(SP, "tp"),
        P(SP, "tp"),
        P(SP, "tp"),
        P(SP, "tp"),
    )
    return jax.shard_map(step, mesh=split, in_specs=in_specs, out_specs=out_specs, check_vma=False)
```
